256 devices in a mesh: sp: 32 (over z, x), tp: 8 (over y, core).
Axes of the slice: x: 4, y: 4, z: 8, core: 2. Of those that a mesh axis runs over, the one named last changes fastest.
Arguments:
- tokens: bfloat16 [16384, 2048], P(('sp', 'tp')), may hold values from -6 to 6
- norm_gain: float32 [2048], replicated, may hold values from 0.1 to 1.9
- rec_query: bfloat16 [2048, 1024], P(None, 'tp'), may hold values from -0.125 to 0.125
- fwd_gate: bfloat16 [2048, 1024], P(None, 'tp'), may hold values from -0.125 to 0.125
- bwd_gate: bfloat16 [2048, 1024], P(None, 'tp'), may hold values from -0.125 to 0.125
- rec_value: bfloat16 [2048, 1024], P(None, 'tp'), may hold values from -0.125 to 0.125
- gate_leak: float32 [2, 1024], P(None, 'tp'), may hold values from 0 to 0.08, as said below
- log_decay: float32 [2, 16384, 8], P(None, 'sp', 'tp'), may hold values from -2.2 to 0, as said below
- rec_gain: float32 [128], replicated, may hold values from 0.1 to 1.9
- att_query: bfloat16 [2048, 1024], P(None, 'tp'), as said below
- att_key: bfloat16 [2048, 1024], P(None, 'tp')
- att_value: bfloat16 [2048, 1024], P(None, 'tp'), may hold values from -0.125 to 0.125
- lambdas: float32 [8], P('tp'), may hold values from 0.3 to 0.8
- att_gain: float32 [128], replicated, may hold values from 0.1 to 1.9
- out_rec: bfloat16 [1024, 2048], replicated, may hold values from -0.125 to 0.125
- out_att: bfloat16 [1024, 2048], replicated, may hold values from -0.125 to 0.125
Outputs:
- layer_out: bfloat16 [16384, 2048], P(('sp', 'tp'))
The draws below stay inside these ranges and needn't reach their ends.
Inputs may be any that keep to these rules, and one draw needn't show every extreme that they name: `gate_leak`: positive, by direction and channel. `log_decay`: never positive. `att_query`: entries of order 2048 to the power -1/2.
All inputs are finite; a program needn't handle non-finite values.
Results may differ from the reference program's by a relative error of at most 0.011.
Values may be sent and summed in bfloat16 or wider, within the bound.
No kernel may reach another device: no remote copies, remote signals or barrier semaphores. Data moves between devices by JAX's collectives and lax.ppermute only.
A program may use at most 128 MiB of HBM per device.

```python
import jax
import jax.numpy as jnp
from jax import lax

D = 2048
HR = 8
HK = 128
HV = 128
HA = 8
AK = 64
AV = 128
BLOCK = 64
TOK_DEV = 512
SEQ = 16384


def draw_gate_leak(key, part):
    pick_key, slow_key, fast_key = jax.random.split(jax.random.fold_in(key, 3), 3)
    slow_share = 0.5
    slow_heads = jax.random.uniform(pick_key, (2, HR, 1), jnp.float32) < slow_share
    slow_rates = jnp.exp(jax.random.uniform(slow_key, (2, HR, HK), jnp.float32, jnp.log(0.3), jnp.log(1.0))) / SEQ
    fast_rates = jnp.exp(jax.random.uniform(fast_key, (2, HR, HK), jnp.float32, jnp.log(0.03), jnp.log(0.08)))
    return jnp.where(slow_heads, slow_rates, fast_rates).reshape(2, HR * HK)


def draw_log_decay(key, part):
    rate_key, spot_key, depth_key = jax.random.split(jax.random.fold_in(key, 5), 3)
    low_rate = 0.3
    high_rate = 1.2
    block_count = SEQ // TOK_DEV
    rates = jnp.exp(jax.random.uniform(rate_key, (2, block_count, 1, HR), jnp.float32, jnp.log(low_rate), jnp.log(high_rate)))
    stable_baseline = jnp.broadcast_to(-rates / SEQ, (2, block_count, TOK_DEV, HR)).reshape(2, SEQ, HR)
    marked_locations = jax.random.randint(spot_key, (2, 3, 1, HR), 0, SEQ)
    layer_depth_list = jax.random.uniform(depth_key, (2, 3, 1, HR), jnp.float32, jnp.log(0.5), jnp.log(0.8))
    token_locations = jnp.arange(SEQ, dtype=jnp.int32)[None, None, :, None]
    spike_events = jnp.sum(jnp.where(token_locations == marked_locations, layer_depth_list, 0.0), axis=1)
    return stable_baseline + spike_events


def attention_pair(key):
    base_key, own_key = jax.random.split(jax.random.fold_in(key, 7), 2)
    columns = HA * 2 * AK
    query_table = jax.random.normal(base_key, (D, columns), jnp.float32) * (3.0 / D) ** 0.5
    key_table = jax.random.normal(own_key, (D, columns), jnp.float32) / D ** 0.5
    return (query_table, key_table)


def draw_att_query(key, part):
    return attention_pair(key)[0].astype(jnp.bfloat16)


def draw_att_key(key, part):
    return attention_pair(key)[1].astype(jnp.bfloat16)


def shard_levels(key, extent, pieces, low, largest):
    factor_of, own = 1.0, jax.random.fold_in(key, 6)
    for dim, blocks in pieces:
        draws = jnp.exp(jax.random.uniform(jax.random.fold_in(own, dim), (blocks,), jnp.float32, low / len(pieces), largest / len(pieces)))
        factor_of = factor_of * jnp.repeat(draws, extent[dim] // blocks).reshape([-1 if axis == dim else 1 for axis in range(len(extent))])
    return factor_of


def bell_draw(rng, extent, deviation, limit, pieces=(), kind=jnp.bfloat16):
    level = shard_levels(rng, extent, pieces, -0.22, 0.18) if pieces else 1.0
    result = jax.random.normal(rng, extent, jnp.float32) * deviation * level
    return jnp.minimum(jnp.maximum(result, -limit), limit).astype(kind)


def setup_inputs(seed: int = 0) -> dict:
    arg_keys = jax.random.split(jax.random.key(seed), 17)
    return {
        "tokens": bell_draw(arg_keys[0], (SEQ, D), 1.0, 6.0, ((0, 256),)),
        "norm_gain": jnp.clip(1.0 + 0.18 * jax.random.normal(arg_keys[1], (D,), jnp.float32), 0.1, 1.9),
        "rec_query": bell_draw(arg_keys[2], (D, HR * HK), D ** -0.5, 0.125, ((1, 8),)),
        "fwd_gate": bell_draw(arg_keys[3], (D, HR * HK), D ** -0.5, 0.125, ((1, 8),)),
        "bwd_gate": bell_draw(arg_keys[4], (D, HR * HK), D ** -0.5, 0.125, ((1, 8),)),
        "rec_value": bell_draw(arg_keys[5], (D, HR * HV), D ** -0.5, 0.125, ((1, 8),)),
        "gate_leak": draw_gate_leak(jax.random.fold_in(arg_keys[16], 71), 0),
        "log_decay": draw_log_decay(jax.random.fold_in(arg_keys[16], 71), 0),
        "rec_gain": jnp.clip(1.0 + 0.18 * jax.random.normal(arg_keys[8], (HV,), jnp.float32), 0.1, 1.9),
        "att_query": draw_att_query(jax.random.fold_in(arg_keys[16], 71), 0),
        "att_key": draw_att_key(jax.random.fold_in(arg_keys[16], 71), 0),
        "att_value": bell_draw(arg_keys[11], (D, HA * AV), D ** -0.5, 0.125, ((1, 8),)),
        "lambdas": jnp.clip(0.3 + 0.5 * jax.random.uniform(arg_keys[12], (HA,), jnp.float32) ** shard_levels(arg_keys[12], (HA,), ((0, 8),), -0.2, 0.2), 0.3, 0.8),
        "att_gain": jnp.clip(1.0 + 0.18 * jax.random.normal(arg_keys[13], (AV,), jnp.float32), 0.1, 1.9),
        "out_rec": bell_draw(arg_keys[14], (HR * HV, D), (HR * HV + HA * AV) ** -0.5, 0.125),
        "out_att": bell_draw(arg_keys[15], (HA * AV, D), (HR * HV + HA * AV) ** -0.5, 0.125),
    }


EPS = 1e-06
THETA = 500000.0
HIGHEST = lax.Precision.HIGHEST

def rms_scale(values, gain):
    return values * lax.rsqrt(lax.optimization_barrier(jnp.mean(values * values, axis=-1, keepdims=True)) + EPS) * gain

def block_recurrence(queries, keys_in, values, log_forget):
    head_count, length, key_width = queries.shape
    value_width = values.shape[-1]
    block_count = length // BLOCK
    block_shape = (head_count, block_count, BLOCK, key_width)
    query_blocks = queries.reshape(block_shape)
    key_blocks = keys_in.reshape(block_shape)
    value_blocks = values.reshape(head_count, block_count, BLOCK, value_width)
    cumulative = jnp.cumsum(log_forget.reshape(block_shape), axis=2)
    middle = cumulative[:, :, BLOCK // 2 - 1:BLOCK // 2]
    block_last = cumulative[:, :, BLOCK - 1:]
    scores = jnp.einsum('hntd,hnsd->hnts', query_blocks * jnp.exp(cumulative - middle), key_blocks * jnp.exp(middle - cumulative), precision=HIGHEST)
    causal_mask = jnp.arange(BLOCK)[:, None] >= jnp.arange(BLOCK)[None, :]
    scores = jnp.where(causal_mask, scores, 0.0)
    within_out = jnp.einsum('hnts,hnsv->hntv', scores, value_blocks, precision=HIGHEST)
    per_block_state = jnp.einsum('hnsd,hnsv->hndv', key_blocks * jnp.exp(block_last - cumulative), value_blocks, precision=HIGHEST)
    block_decay = jnp.exp(block_last[:, :, 0])

    def advance(running, inputs_now):
        factor, added_state = inputs_now
        return (factor[..., None] * running + added_state, running)
    initial = jnp.zeros((head_count, key_width, value_width), jnp.float32)
    end_state, before = lax.scan(advance, initial, (jnp.moveaxis(block_decay, 1, 0), jnp.moveaxis(per_block_state, 1, 0)))
    before = jnp.moveaxis(before, 0, 1)
    carried = jnp.einsum('hntd,hndv->hntv', query_blocks * jnp.exp(cumulative), before, precision=HIGHEST)
    return ((within_out + carried).reshape(head_count, length, value_width), end_state, cumulative)

def rotate(vectors, positions):
    half_width = AK // 2
    frequency = THETA ** (-(jnp.arange(half_width, dtype=jnp.float32) * 2.0 / AK))
    angles = positions[:, None] * frequency[None, :]
    cosine = jnp.cos(angles)[:, None, None, :]
    sines = jnp.sin(angles)[:, None, None, :]
    first_half = vectors[..., :half_width]
    second = vectors[..., half_width:]
    return jnp.concatenate([first_half * cosine - second * sines, second * cosine + first_half * sines], axis=-1)

def reference(tokens, norm_gain, rec_query, fwd_gate, bwd_gate, rec_value, gate_leak, log_decay, rec_gain, att_query, att_key, att_value, lambdas, att_gain, out_rec, out_att):
    normed = rms_scale(tokens.astype(jnp.float32), norm_gain).astype(jnp.bfloat16)

    def project(weight):
        return jnp.dot(normed, weight, preferred_element_type=jnp.float32).astype(jnp.bfloat16)

    def split_heads(table, width):
        return table.astype(jnp.float32).reshape(SEQ, -1, width).transpose(1, 0, 2)
    queries = jax.nn.silu(split_heads(project(rec_query), HK))
    values = split_heads(project(rec_value), HV)
    key_fwd = gate_leak[0].reshape(HR, 1, HK) * jax.nn.sigmoid(-split_heads(project(fwd_gate), HK))
    key_bwd = gate_leak[1].reshape(HR, 1, HK) * jax.nn.sigmoid(-split_heads(project(bwd_gate), HK))
    log_fwd = jnp.log1p(-key_fwd) + log_decay[0].T[:, :, None]
    log_bwd = jnp.log1p(-key_bwd) + log_decay[1].T[:, :, None]
    out_fwd = block_recurrence(queries, key_fwd, values, log_fwd)[0]
    flipped = block_recurrence(jnp.flip(queries, 1), jnp.flip(key_bwd, 1), jnp.flip(values, 1), jnp.flip(log_bwd, 1))[0]
    rec_rows = rms_scale(out_fwd + jnp.flip(flipped, 1), rec_gain)
    rec_rows = rec_rows.transpose(1, 0, 2).reshape(SEQ, HR * HV).astype(jnp.bfloat16)
    positions = jnp.arange(SEQ, dtype=jnp.int32).astype(jnp.float32)
    att_queries = (rotate(project(att_query).astype(jnp.float32).reshape(SEQ, HA, 2, AK), positions) * AK ** (-0.5)).astype(jnp.bfloat16)
    att_keys = rotate(project(att_key).astype(jnp.float32).reshape(SEQ, HA, 2, AK), positions).astype(jnp.bfloat16)
    att_values = project(att_value).reshape(SEQ, HA, AV)

    def attend_head(inputs_now):
        head_queries, head_keys, head_values, weight = inputs_now
        keys_wide = head_keys.astype(jnp.float32)
        values_wide = head_values.astype(jnp.float32)

        def attend_rows(query_block):
            scores = jnp.einsum('qmd,kmd->mqk', query_block.astype(jnp.float32), keys_wide, precision=HIGHEST)
            weights_raw = jnp.exp(scores - lax.optimization_barrier(jnp.max(scores, axis=-1, keepdims=True)))
            totals = lax.optimization_barrier(jnp.sum(weights_raw, axis=-1))
            rounded = lax.optimization_barrier(weights_raw.astype(jnp.bfloat16)).astype(jnp.float32)
            summed = jnp.einsum('mqk,kv->mqv', rounded, values_wide, precision=HIGHEST)
            return summed[0] / totals[0][:, None] - weight * summed[1] / totals[1][:, None]
        blocks = head_queries.reshape(SEQ // TOK_DEV, TOK_DEV, 2, AK)
        return lax.map(attend_rows, blocks).reshape(SEQ, AV)
    mixed_heads = lax.map(attend_head, (jnp.moveaxis(att_queries, 1, 0), jnp.moveaxis(att_keys, 1, 0), jnp.moveaxis(att_values, 1, 0), lambdas))
    att_rows = rms_scale(mixed_heads, att_gain).transpose(1, 0, 2).reshape(SEQ, HA * AV).astype(jnp.bfloat16)
    projected = jnp.dot(rec_rows, out_rec, preferred_element_type=jnp.float32) + jnp.dot(att_rows, out_att, preferred_element_type=jnp.float32)
    return projected.astype(jnp.bfloat16)
```

```python
import functools

import jax
import jax.numpy as jnp
from jax import lax
from jax.experimental import pallas as pl
from jax.experimental.pallas import tpu as pltpu
from jax.sharding import Mesh
from jax.sharding import PartitionSpec as P

HK = 128
HV = 128
AK = 64
AV = 128
BLOCK = 64
NZ, NX, NY, NC = 8, 4, 4, 2
AXES = ("z", "x", "y", "c")
SP = ("z", "x")
TP = ("y", "c")
TOK = 512
ACC_ROWS = 144
SEND_ROWS = 2 * AV + 16
BF16 = jnp.bfloat16
F32 = jnp.float32

EPS = 1e-06
THETA = 500000.0
LOW = -1e30


def shift(value, axis, by, size):
    return lax.ppermute(value, axis, [(i, (i + by) % size) for i in range(size)])


def gather_rows(rows):
    y, c = lax.axis_index("y"), lax.axis_index("c")
    half = rows.shape[0] // 2
    up = shift(rows, "y", 1, NY)
    down = shift(rows, "y", -1, NY)
    far_low = shift(rows[:half], "y", 2, NY)
    far_high = shift(rows[half:], "y", -2, NY)
    mine = jnp.zeros((NY, *rows.shape), rows.dtype)
    for piece, source in (
        (rows, y),
        (up, (y + 3) % 4),
        (down, (y + 1) % 4),
        (jnp.concatenate([far_low, far_high]), (y + 2) % 4),
    ):
        mine = lax.dynamic_update_slice(mine, piece[None], (source, 0, 0))
    other = shift(mine, "c", 1, NC)
    both = jnp.zeros((NY, NC, *rows.shape), rows.dtype)
    both = lax.dynamic_update_slice(both, mine[:, None], (0, c, 0, 0))
    both = lax.dynamic_update_slice(both, other[:, None], (0, 1 - c, 0, 0))
    return both.reshape(-1, rows.shape[1])


def rms_scale(values, gain):
    return values * lax.rsqrt(jnp.mean(values * values, axis=-1, keepdims=True) + EPS) * gain


def block_recurrence(queries, keys_in, values, log_forget):
    head_count, length, key_width = queries.shape
    value_width = values.shape[-1]
    block_count = length // BLOCK
    block_shape = (head_count, block_count, BLOCK, key_width)
    query_blocks = queries.reshape(block_shape)
    key_blocks = keys_in.reshape(block_shape)
    value_blocks = values.reshape(head_count, block_count, BLOCK, value_width)
    cumulative = jnp.cumsum(log_forget.reshape(block_shape), axis=2)
    middle = cumulative[:, :, BLOCK // 2 - 1 : BLOCK // 2]
    block_last = cumulative[:, :, BLOCK - 1 :]
    scores = jnp.einsum(
        "hntd,hnsd->hnts",
        query_blocks * jnp.exp(cumulative - middle),
        key_blocks * jnp.exp(middle - cumulative),
    )
    causal_mask = jnp.arange(BLOCK)[:, None] >= jnp.arange(BLOCK)[None, :]
    scores = jnp.where(causal_mask, scores, 0.0)
    within_out = jnp.einsum("hnts,hnsv->hntv", scores, value_blocks)
    per_block_state = jnp.einsum(
        "hnsd,hnsv->hndv", key_blocks * jnp.exp(block_last - cumulative), value_blocks
    )
    block_decay = jnp.exp(block_last[:, :, 0])

    def advance(running, inputs_now):
        factor, added_state = inputs_now
        return (factor[..., None] * running + added_state, running)

    initial = jnp.zeros((head_count, key_width, value_width), jnp.float32)
    end_state, before = lax.scan(
        advance, initial, (jnp.moveaxis(block_decay, 1, 0), jnp.moveaxis(per_block_state, 1, 0))
    )
    before = jnp.moveaxis(before, 0, 1)
    carried = jnp.einsum("hntd,hndv->hntv", query_blocks * jnp.exp(cumulative), before)
    return ((within_out + carried).reshape(head_count, length, value_width), end_state, cumulative)


def local_direction(queries, keys_in, values, log_forget):
    outputs, end_state, cumulative = block_recurrence(queries, keys_in, values, log_forget)
    head_count, length, key_width = queries.shape
    block_totals = cumulative[:, :, BLOCK - 1]
    before_block = jnp.cumsum(block_totals, axis=1) - block_totals
    within = (cumulative + before_block[:, :, None]).reshape(head_count, length, key_width)
    return (outputs, jnp.exp(jnp.sum(block_totals, axis=1)), end_state, queries * jnp.exp(within))


def rotate(vectors, positions):
    half_width = AK // 2
    frequency = THETA ** (-(jnp.arange(half_width, dtype=jnp.float32) * 2.0 / AK))
    angles = positions[:, None] * frequency[None, :]
    cosine = jnp.cos(angles)[:, None, :]
    sines = jnp.sin(angles)[:, None, :]
    first_half = vectors[..., :half_width]
    second = vectors[..., half_width:]
    return jnp.concatenate(
        [first_half * cosine - second * sines, second * cosine + first_half * sines], axis=-1
    )


def attend_body(*refs, first, last, chunks, key_block):
    q_ref, *kv_refs = refs[: 1 + chunks]
    rest = refs[1 + chunks :]
    if not first:
        peak_in, acc_in = rest[:2]
        rest = rest[2:]
    if last:
        send_ref, k_all, v_all, peaks, accs = rest
    else:
        peaks, accs, k_all, v_all = rest
    width = q_ref.shape[-1]
    rows = kv_refs[0].shape[0]

    @pl.when(pl.program_id(0) == 0)
    def _():
        for n, kv in enumerate(kv_refs):
            k_all[n * rows : (n + 1) * rows, :] = kv[:, :128]
            v_all[:AV, n * rows : (n + 1) * rows] = kv[:, 128:].T
        v_all[AV:, :] = jnp.ones((ACC_ROWS - AV, chunks * rows), BF16)

    if first:
        peaks[...] = jnp.full(peaks.shape, LOW, F32)
        accs[...] = jnp.zeros(accs.shape, F32)
    else:
        peaks[...] = peak_in[...]
        accs[...] = acc_in[...]
    both = q_ref[...]
    upper = lax.broadcasted_iota(jnp.int32, (2 * AK, width), 0) < AK
    zero = jnp.zeros_like(both)
    maps = (jnp.where(upper, both, zero), jnp.where(upper, zero, both))

    def absorb(i, unused):
        at = pl.multiple_of(i * key_block, key_block)
        keys = k_all[pl.ds(at, key_block), :]
        values = v_all[:, pl.ds(at, key_block)]
        scores = [jnp.dot(keys, q, preferred_element_type=F32) for q in maps]
        for m in range(2):
            old = peaks[m, 0:1, :]
            new = jnp.maximum(old, jnp.max(scores[m], axis=0, keepdims=True))
            weights = jnp.exp(scores[m] - new).astype(BF16)
            accs[m] = accs[m] * jnp.exp(old - new) + jnp.dot(
                values, weights, preferred_element_type=F32
            )
            peaks[m, 0:1, :] = new
        return 0

    lax.fori_loop(0, chunks * rows // key_block, absorb, 0, unroll=2)
    if last:
        for m in range(2):
            acc = accs[m]
            total = acc[AV : AV + 1, :]
            send_ref[0, m * AV : (m + 1) * AV, :] = (acc[:AV] / total).astype(BF16)
            level = peaks[m, 0:1, :] + jnp.log(total)
            high = level.astype(BF16)
            left = level - high.astype(F32)
            middle = left.astype(BF16)
            low = (left - middle.astype(F32)).astype(BF16)
            at = 2 * AV + 8 * m
            send_ref[0, at : at + 8, :] = jnp.concatenate(
                [high.astype(F32), middle.astype(F32), low.astype(F32), jnp.zeros((5, width), F32)]
            ).astype(BF16)


def attend(queries, pieces, state=None, last=False):
    chunks, rows = len(pieces), pieces[0].shape[0]
    count = queries.shape[1]
    tiles = count // TOK
    first = state is None
    kv_spec = pl.BlockSpec((rows, 256), lambda i: (0, 0))
    peak_spec = pl.BlockSpec((2, 8, TOK), lambda i: (0, 0, i))
    acc_spec = pl.BlockSpec((2, ACC_ROWS, TOK), lambda i: (0, 0, i))
    in_specs = [pl.BlockSpec((2 * AK, TOK), lambda i: (0, i))] + [kv_spec] * chunks
    operands = [queries, *pieces]
    if not first:
        in_specs += [peak_spec, acc_spec]
        operands += state
    scratch = [pltpu.VMEM((chunks * rows, 128), BF16), pltpu.VMEM((ACC_ROWS, chunks * rows), BF16)]
    if last:
        out_specs = [pl.BlockSpec((1, SEND_ROWS, TOK), lambda i: (i, 0, 0))]
        out_shape = [jax.ShapeDtypeStruct((tiles, SEND_ROWS, TOK), BF16)]
        scratch += [pltpu.VMEM((2, 8, TOK), F32), pltpu.VMEM((2, ACC_ROWS, TOK), F32)]
    else:
        out_specs = [peak_spec, acc_spec]
        out_shape = [
            jax.ShapeDtypeStruct((2, 8, count), F32),
            jax.ShapeDtypeStruct((2, ACC_ROWS, count), F32),
        ]
    body = functools.partial(attend_body, first=first, last=last, chunks=chunks, key_block=TOK)
    work = 2 * count * chunks * rows
    return pl.pallas_call(
        body,
        grid=(tiles,),
        in_specs=in_specs,
        out_specs=out_specs,
        out_shape=out_shape,
        scratch_shapes=scratch,
        cost_estimate=pl.CostEstimate(
            flops=work * 2 * (AK + AV), transcendentals=work, bytes_accessed=count * 2048
        ),
        compiler_params=pltpu.CompilerParams(vmem_limit_bytes=48 * 1024 * 1024),
        name="attend",
    )(*operands)


def mix_body(a_ref, b_ref, c_ref, d_ref, weight_ref, gain_ref, out_ref):
    refs = (a_ref, b_ref, c_ref, d_ref)
    mixed = None
    for m in range(2):
        at = 2 * AV + 8 * m
        levels = []
        for ref in refs:
            parts = ref[at : at + 8, :].astype(F32)
            levels.append(parts[0:1] + parts[1:2] + parts[2:3])
        peak = functools.reduce(jnp.maximum, levels)
        shares = [jnp.exp(level - peak) for level in levels]
        total = functools.reduce(jnp.add, shares)
        summed = None
        for ref, share in zip(refs, shares):
            term = ref[m * AV : (m + 1) * AV, :].astype(F32) * (share / total)
            summed = term if summed is None else summed + term
        mixed = summed if m == 0 else mixed - weight_ref[0] * summed
    scale = lax.rsqrt(jnp.mean(mixed * mixed, axis=0, keepdims=True) + EPS)
    out_ref[...] = ((mixed * scale).T * gain_ref[...]).astype(BF16)


def mix(partials, weight, gain):
    vmem = pl.BlockSpec(memory_space=pltpu.VMEM)
    return pl.pallas_call(
        mix_body,
        in_specs=[vmem] * 4 + [pl.BlockSpec(memory_space=pltpu.SMEM), vmem],
        out_specs=vmem,
        out_shape=jax.ShapeDtypeStruct((TOK, AV), BF16),
        name="mix",
    )(*partials, weight, gain.reshape(1, AV))


def link(earlier, later):
    return (earlier[0] * later[0], later[0][..., None] * earlier[1] + later[1])


def fold(entries, passed, order):
    decay = jnp.ones((HK,), F32)
    state = jnp.zeros((HK, HV), F32)
    for k in order:
        new = link((decay, state), entries[k])
        decay = jnp.where(passed[k], new[0], decay)
        state = jnp.where(passed[k], new[1], state)
    return decay, state


def along(value, axis, size):
    return [value] + [shift(value, axis, k, size) for k in range(1, size)]


def entering_states(fwd, bwd):
    def pack(f, b):
        return jnp.concatenate([f[1], b[1], f[0][None], b[0][None], jnp.zeros((6, HV), F32)]).astype(BF16)

    def unpack(p):
        p = p.astype(F32)
        return (p[2 * HK], p[:HK]), (p[2 * HK + 1], p[HK : 2 * HK])

    before = after = None
    subtotal = (fwd, bwd)
    for axis, size in (("x", NX), ("z", NZ)):
        place = lax.axis_index(axis)
        entries = [unpack(p) for p in along(pack(*subtotal), axis, size)]
        below = [(k <= place) & (k > 0) for k in range(size)]
        above = [k > place for k in range(size)]
        f_below = fold([e[0] for e in entries], below, range(size - 1, 0, -1))
        b_above = fold([e[1] for e in entries], above, range(1, size))
        if before is None:
            f_above = fold([e[0] for e in entries], above, range(size - 1, 0, -1))
            b_below = fold([e[1] for e in entries], below, range(1, size))
            subtotal = (
                link(link(f_below, entries[0][0]), f_above),
                link(link(b_above, entries[0][1]), b_below),
            )
            before, after = f_below, b_above
        else:
            before = link(f_below, before)
            after = link(b_above, after)
    return before[1], after[1]


def on_device(
    tokens,
    norm_gain,
    rec_query,
    fwd_gate,
    bwd_gate,
    rec_value,
    gate_leak,
    log_decay,
    rec_gain,
    att_query,
    att_key,
    att_value,
    lambdas,
    att_gain,
    out_rec,
    out_att,
):
    normed = rms_scale(tokens.astype(F32), norm_gain).astype(BF16)
    weights_all = (att_key, att_value, att_query, rec_query, fwd_gate, bwd_gate, rec_value)
    joined = jnp.concatenate(weights_all, axis=1)
    projected = jnp.dot(gather_rows(normed), joined, preferred_element_type=F32).astype(BF16)
    length = projected.shape[0]
    att_key_raw, att_value_raw, att_query_raw, query_raw, fwd_raw, bwd_raw, value_raw = jnp.split(
        projected, 7, axis=1
    )
    positions = (lax.axis_index(SP) * length + jnp.arange(length, dtype=jnp.int32)).astype(F32)
    att_keys = rotate(att_key_raw.astype(F32).reshape(length, 2, AK), positions).astype(BF16)
    own_kv = jnp.concatenate([att_keys.reshape(length, 2 * AK), att_value_raw], axis=1)
    att_queries = (
        rotate(att_query_raw.astype(F32).reshape(length, 2, AK), positions) * AK ** (-0.5)
    ).astype(BF16)
    own_q = att_queries.reshape(length, 2 * AK).T

    queries_all = jnp.concatenate(
        [own_q, shift(own_q, "x", 1, NX), shift(own_q, "x", -1, NX), shift(own_q, "x", 2, NX)],
        axis=1,
    )
    ups, downs = [own_kv], [own_kv]
    for step in range(NZ // 2):
        ups.append(shift(ups[-1], "z", 1, NZ))
        if step < NZ // 2 - 1:
            downs.append(shift(downs[-1], "z", -1, NZ))

    def split_heads(table):
        return table.astype(F32)[None]

    queries = jax.nn.silu(split_heads(query_raw))
    values = split_heads(value_raw)
    key_fwd = gate_leak[0] * jax.nn.sigmoid(-split_heads(fwd_raw))
    key_bwd = gate_leak[1] * jax.nn.sigmoid(-split_heads(bwd_raw))
    log_fwd = jnp.log1p(-key_fwd) + log_decay[0].T[:, :, None]
    log_bwd = jnp.log1p(-key_bwd) + log_decay[1].T[:, :, None]
    out_fwd, decay_fwd, ending_fwd, read_fwd = local_direction(queries, key_fwd, values, log_fwd)
    out_back, decay_bwd, ending_bwd, read_bwd = local_direction(
        jnp.flip(queries, 1), jnp.flip(key_bwd, 1), jnp.flip(values, 1), jnp.flip(log_bwd, 1)
    )
    entry_fwd, entry_bwd = entering_states(
        (decay_fwd[0], ending_fwd[0]), (decay_bwd[0], ending_bwd[0])
    )

    state = attend(queries_all, [ups[0], ups[1], downs[1]])
    state = attend(queries_all, [ups[2], downs[2]], state)
    sends = attend(queries_all, [ups[3], downs[3], ups[4]], state, last=True)[0]
    partials = [
        sends[0],
        shift(sends[1], "x", -1, NX),
        shift(sends[2], "x", 1, NX),
        shift(sends[3], "x", -2, NX),
    ]
    att_rows = mix(partials, lambdas, att_gain)

    out_fwd = out_fwd[0] + jnp.dot(read_fwd[0], entry_fwd)
    out_back = out_back[0] + jnp.dot(read_bwd[0], entry_bwd)
    rec_rows = rms_scale(out_fwd + jnp.flip(out_back, 0), rec_gain).astype(BF16)
    rows = jnp.stack([rec_rows, att_rows], axis=1).reshape(8, length // 8, 2, HV)
    swapped = lax.all_to_all(rows, TP, split_axis=0, concat_axis=0, tiled=True)
    rec_all = swapped[:, :, 0].transpose(1, 0, 2).reshape(length // 8, -1)
    att_all = swapped[:, :, 1].transpose(1, 0, 2).reshape(length // 8, -1)
    projected_out = jnp.dot(rec_all, out_rec, preferred_element_type=F32) + jnp.dot(
        att_all, out_att, preferred_element_type=F32
    )
    return projected_out.astype(BF16)


def solution(mesh):
    torus = Mesh(mesh.devices.reshape(NZ, NX, NY, NC), AXES)
    in_specs = (
        P(AXES, None),
        P(),
        P(None, TP),
        P(None, TP),
        P(None, TP),
        P(None, TP),
        P(None, TP),
        P(None, SP, TP),
        P(),
        P(None, TP),
        P(None, TP),
        P(None, TP),
        P(TP),
        P(),
        P(),
        P(),
    )
    out_specs = P(AXES, None)
    return jax.shard_map(
        on_device, mesh=torus, in_specs=in_specs, out_specs=out_specs, check_vma=False
    )
```

```python
import functools

import jax
import jax.numpy as jnp
from jax import lax
from jax.experimental import pallas as pl
from jax.experimental.pallas import tpu as pltpu
from jax.sharding import Mesh
from jax.sharding import PartitionSpec as P


HK = 128
HV = 128
AK = 64
AV = 128
BLOCK = 64
NZ, NX, NY, NC = 8, 4, 4, 2
AXES = ("z", "x", "y", "c")
SP = ("z", "x")
TP = ("y", "c")
TOK = 512
ACC_ROWS = 144
SEND_ROWS = 2 * AV + 16
PACK = 784
BF16 = jnp.bfloat16
F32 = jnp.float32

EPS = 1e-06
THETA = 500000.0
LOW = -1e30


def shift(value, axis, by, size):
    return lax.ppermute(value, axis, [(i, (i + by) % size) for i in range(size)])


def gather_rows(rows):
    y, c = lax.axis_index("y"), lax.axis_index("c")
    half = rows.shape[0] // 2
    up = shift(rows, "y", 1, NY)
    down = shift(rows, "y", -1, NY)
    far_low = shift(rows[:half], "y", 2, NY)
    far_high = shift(rows[half:], "y", -2, NY)
    mine = jnp.zeros((NY, *rows.shape), rows.dtype)
    for piece, source in (
        (rows, y),
        (up, (y + 3) % 4),
        (down, (y + 1) % 4),
        (jnp.concatenate([far_low, far_high]), (y + 2) % 4),
    ):
        mine = lax.dynamic_update_slice(mine, piece[None], (source, 0, 0))
    other = shift(mine, "c", 1, NC)
    both = jnp.zeros((NY, NC, *rows.shape), rows.dtype)
    both = lax.dynamic_update_slice(both, mine[:, None], (0, c, 0, 0))
    both = lax.dynamic_update_slice(both, other[:, None], (0, 1 - c, 0, 0))
    return both.reshape(-1, rows.shape[1])


def rms_scale(values, gain):
    return values * lax.rsqrt(jnp.mean(values * values, axis=-1, keepdims=True) + EPS) * gain


VMEM = pl.BlockSpec(memory_space=pltpu.VMEM)
SMEM = pl.BlockSpec(memory_space=pltpu.SMEM)


def columns(n):
    return pl.BlockSpec((TOK, 128), lambda *_: (0, n))


def cost(flops, transcendentals=0):
    return pl.CostEstimate(flops=flops, transcendentals=transcendentals, bytes_accessed=1 << 20)


def rotation_tables(length):
    positions = (lax.axis_index(SP) * length + jnp.arange(length, dtype=jnp.int32)).astype(F32)
    frequency = THETA ** (-(jnp.arange(AK // 2, dtype=F32) * 2.0 / AK))
    angles = positions[:, None] * frequency[None, :]
    cosine, sine = jnp.cos(angles), jnp.sin(angles)
    return (
        jnp.concatenate([cosine] * 4, axis=1),
        jnp.concatenate([-sine, sine, -sine, sine], axis=1),
    )


def rotated(vectors, cosine, sine):
    lane = lax.broadcasted_iota(jnp.int32, vectors.shape, 1)
    half = AK // 2
    partner = jnp.where(
        (lane & half) == 0, pltpu.roll(vectors, 128 - half, 1), pltpu.roll(vectors, half, 1)
    )
    return vectors * cosine + partner * sine


def keys_body(key_ref, value_ref, cos_ref, sin_ref, out_ref):
    out_ref[:, :128] = rotated(key_ref[...].astype(F32), cos_ref[...], sin_ref[...]).astype(BF16)
    out_ref[:, 128:] = value_ref[...]


def make_keys(projected, cosine, sine):
    table = pl.BlockSpec((TOK, 128), lambda i: (0, 0))
    return pl.pallas_call(
        keys_body,
        grid=(1,),
        in_specs=[columns(0), columns(1), table, table],
        out_specs=pl.BlockSpec((TOK, 256), lambda i: (0, 0)),
        out_shape=jax.ShapeDtypeStruct((TOK, 256), BF16),
        cost_estimate=cost(1 << 22),
        name="make_keys",
    )(projected, projected, cosine, sine)


def local_body(
    aq_ref, q_ref, f_ref, b_ref, v_ref, leak_ref, decay_ref, cos_ref, sin_ref,
    pack_ref, out_ref, read_f_ref, read_b_ref,
):
    pack_ref[:TOK, :] = (
        rotated(aq_ref[...].astype(F32), cos_ref[...], sin_ref[...]) * AK ** (-0.5)
    ).astype(BF16)
    raw = q_ref[...].astype(F32)
    queries = raw / (1.0 + jnp.exp(-raw))
    row = lax.broadcasted_iota(jnp.int32, (BLOCK, BLOCK), 0)
    col = lax.broadcasted_iota(jnp.int32, (BLOCK, BLOCK), 1)
    totals = []
    for way, (gate_ref, read_ref) in enumerate(((f_ref, read_f_ref), (b_ref, read_b_ref))):
        keys = leak_ref[way : way + 1, :] / (1.0 + jnp.exp(gate_ref[...].astype(F32)))
        logs = jnp.log1p(-keys) + decay_ref[way]
        reach = (row >= col) if way == 0 else (row <= col)
        sums = jnp.where(reach, 1.0, 0.0)
        middle_row, last_row = (BLOCK // 2 - 1, BLOCK - 1) if way == 0 else (BLOCK // 2, 0)
        state = jnp.zeros((HV, HK), F32)
        before = jnp.zeros((1, HK), F32)
        blocks = range(TOK // BLOCK)
        for n in blocks if way == 0 else reversed(blocks):
            at = slice(n * BLOCK, (n + 1) * BLOCK)
            cumulative = jnp.dot(
                sums, logs[at], precision=lax.Precision.HIGHEST, preferred_element_type=F32
            )
            middle = cumulative[middle_row : middle_row + 1]
            last = cumulative[last_row : last_row + 1]
            scores = lax.dot_general(
                (queries[at] * jnp.exp(cumulative - middle)).astype(BF16),
                (keys[at] * jnp.exp(middle - cumulative)).astype(BF16),
                (((1,), (1,)), ((), ())),
                preferred_element_type=F32,
            )
            scores = jnp.where(reach, scores, 0.0).astype(BF16)
            values = v_ref[at, :]
            out = jnp.dot(scores, values, preferred_element_type=F32)
            read = queries[at] * jnp.exp(cumulative)
            out = out + lax.dot_general(
                read.astype(BF16),
                state.astype(BF16),
                (((1,), (1,)), ((), ())),
                preferred_element_type=F32,
            )
            out_ref[at, :] = out if way == 0 else out_ref[at, :] + out
            read_ref[at, :] = (read * jnp.exp(before)).astype(BF16)
            added = lax.dot_general(
                values,
                (keys[at] * jnp.exp(last - cumulative)).astype(BF16),
                (((0,), (0,)), ((), ())),
                preferred_element_type=F32,
            )
            state = state * jnp.exp(last) + added
            before = before + last
        pack_ref[TOK + way * HV : TOK + (way + 1) * HV, :] = state.astype(BF16)
        totals.append(jnp.exp(before))
    pack_ref[TOK + 2 * HV :, :] = jnp.concatenate(
        [*totals, jnp.zeros((PACK - TOK - 2 * HV - 2, HK), F32)]
    ).astype(BF16)


def make_local(projected, leak, decays, cosine, sine):
    whole = pl.BlockSpec((TOK, 128), lambda i: (0, 0))
    return pl.pallas_call(
        local_body,
        grid=(1,),
        in_specs=[columns(n) for n in range(2, 7)]
        + [pl.BlockSpec((2, 128), lambda i: (0, 0)), pl.BlockSpec((2, TOK, 128), lambda i: (0, 0, 0)), whole, whole],
        out_specs=[pl.BlockSpec((PACK, 128), lambda i: (0, 0)), whole, whole, whole],
        out_shape=[
            jax.ShapeDtypeStruct((PACK, 128), BF16),
            jax.ShapeDtypeStruct((TOK, 128), F32),
            jax.ShapeDtypeStruct((TOK, 128), BF16),
            jax.ShapeDtypeStruct((TOK, 128), BF16),
        ],
        cost_estimate=cost(1 << 28),
        compiler_params=pltpu.CompilerParams(vmem_limit_bytes=32 * 1024 * 1024),
        name="local",
    )(projected, projected, projected, projected, projected, leak, decays, cosine, sine)


def link(earlier, later):
    return (earlier[0] * later[0], later[0] * earlier[1] + later[1])


def pick(condition, new, old):
    return tuple(jnp.where(condition, a, b) for a, b in zip(new, old))


def read_sent(ref, at):
    decays = ref[at + 2 * HV : at + 2 * HV + 16, :].astype(F32)
    return (
        (decays[0:1], ref[at : at + HV, :].astype(F32)),
        (decays[1:2], ref[at + HV : at + 2 * HV, :].astype(F32)),
    )


def write_sent(ref, fwd, bwd):
    ref[:HV, :] = fwd[1].astype(BF16)
    ref[HV : 2 * HV, :] = bwd[1].astype(BF16)
    ref[2 * HV :, :] = jnp.concatenate([fwd[0], bwd[0], jnp.zeros((14, HK), F32)]).astype(BF16)


def write_kept(ref, n, pair):
    ref[n, :HV, :] = pair[1]
    ref[n, HV:, :] = jnp.broadcast_to(pair[0], (8, HK))


def read_kept(ref, n):
    return ref[n, HV : HV + 1, :], ref[n, :HV, :]


def fold_body(place_ref, own_ref, below1_ref, below2_ref, below3_ref, kept_ref, sent_ref):
    place = place_ref[0]
    entries = [read_sent(ref, TOK) for ref in (own_ref, below1_ref, below2_ref, below3_ref)]
    none = (jnp.ones((1, HK), F32), jnp.zeros((HV, HK), F32))

    def fold(way, below, order):
        found = none
        for k in order:
            passed = (place >= k) if below else (place < k)
            found = pick(passed, link(found, entries[k][way]), found)
        return found

    f_below, f_above = fold(0, True, (3, 2, 1)), fold(0, False, (3, 2, 1))
    b_above, b_below = fold(1, False, (1, 2, 3)), fold(1, True, (1, 2, 3))
    fwd = link(link(f_below, entries[0][0]), f_above)
    bwd = link(link(b_above, entries[0][1]), b_below)
    for n, pair in enumerate((fwd, bwd, f_below, b_above)):
        write_kept(kept_ref, n, pair)
    write_sent(sent_ref, fwd, bwd)


KEPT = jax.ShapeDtypeStruct((4, HV + 8, HK), F32)
SENT = jax.ShapeDtypeStruct((2 * HV + 16, HK), BF16)


def fold_x(place, packs):
    return pl.pallas_call(
        fold_body,
        in_specs=[SMEM] + [VMEM] * 4,
        out_specs=[VMEM, VMEM],
        out_shape=[KEPT, SENT],
        cost_estimate=cost(1 << 22),
        name="fold_x",
    )(place, *packs)


def met(lower, kept_ref, received_ref):
    fwd, bwd, before, after = (read_kept(kept_ref, n) for n in range(4))
    peer_f, peer_b = read_sent(received_ref, 0)
    return (
        pick(lower, link(peer_f, fwd), link(fwd, peer_f)),
        pick(lower, link(bwd, peer_b), link(peer_b, bwd)),
        pick(lower, link(peer_f, before), before),
        pick(lower, after, link(peer_b, after)),
    )


def merge_body(lower_ref, kept_ref, received_ref, out_ref, sent_ref):
    pairs = met(lower_ref[0] == 1, kept_ref, received_ref)
    for n, pair in enumerate(pairs):
        write_kept(out_ref, n, pair)
    write_sent(sent_ref, pairs[0], pairs[1])


def merge(lower, kept, received):
    return pl.pallas_call(
        merge_body,
        in_specs=[SMEM, VMEM, VMEM],
        out_specs=[VMEM, VMEM],
        out_shape=[KEPT, SENT],
        cost_estimate=cost(1 << 22),
        name="merge",
    )(lower, kept, received)


def finish_body(lower_ref, kept_ref, received_ref, out_ref, read_f_ref, read_b_ref, gain_ref, rows_ref):
    _, _, before, after = met(lower_ref[0] == 1, kept_ref, received_ref)
    total = out_ref[...]
    for read_ref, (_, state) in ((read_f_ref, before), (read_b_ref, after)):
        total = total + lax.dot_general(
            read_ref[...], state.astype(BF16), (((1,), (1,)), ((), ())), preferred_element_type=F32
        )
    rows_ref[...] = rms_scale(total, gain_ref[...]).astype(BF16)


def finish(lower, kept, received, out, read_f, read_b, gain):
    return pl.pallas_call(
        finish_body,
        in_specs=[SMEM] + [VMEM] * 6,
        out_specs=VMEM,
        out_shape=jax.ShapeDtypeStruct((TOK, HV), BF16),
        cost_estimate=cost(1 << 25),
        name="finish",
    )(lower, kept, received, out, read_f, read_b, gain.reshape(1, HV))


def attend_body(*refs, first, last, chunks, key_block):
    counts = (4 if first else 1, chunks, 0 if first else 2)
    q_refs, kv_refs, state_in = (
        refs[sum(counts[:n]) : sum(counts[: n + 1])] for n in range(3)
    )
    rest = refs[sum(counts) :]
    if last:
        send_ref, k_all, v_all, peaks, accs = rest
    elif first:
        turned_ref, peaks, accs, k_all, v_all = rest
    else:
        peaks, accs, k_all, v_all = rest
    rows = kv_refs[0].shape[0]
    tile = pl.program_id(0)

    @pl.when(tile == 0)
    def _():
        for n, kv in enumerate(kv_refs):
            k_all[n * rows : (n + 1) * rows, :] = kv[:, :128]
            v_all[:AV, n * rows : (n + 1) * rows] = kv[:, 128:].T
        v_all[AV:, :] = jnp.ones((ACC_ROWS - AV, chunks * rows), BF16)

    if first:
        peaks[...] = jnp.full(peaks.shape, LOW, F32)
        accs[...] = jnp.zeros(accs.shape, F32)
        for n, ref in enumerate(q_refs):

            @pl.when(tile == n)
            def _():
                turned_ref[0] = ref[...].T

        both = turned_ref[0]
    else:
        peaks[...] = state_in[0][...]
        accs[...] = state_in[1][...]
        both = q_refs[0][0]
    width = both.shape[-1]
    upper = lax.broadcasted_iota(jnp.int32, (2 * AK, width), 0) < AK
    zero = jnp.zeros_like(both)
    maps = (jnp.where(upper, both, zero), jnp.where(upper, zero, both))

    def absorb(i, unused):
        at = pl.multiple_of(i * key_block, key_block)
        keys = k_all[pl.ds(at, key_block), :]
        values = v_all[:, pl.ds(at, key_block)]
        scores = [jnp.dot(keys, q, preferred_element_type=F32) for q in maps]
        for m in range(2):
            old = peaks[m, 0:1, :]
            new = jnp.maximum(old, jnp.max(scores[m], axis=0, keepdims=True))
            weights = jnp.exp(scores[m] - new).astype(BF16)
            accs[m] = accs[m] * jnp.exp(old - new) + jnp.dot(
                values, weights, preferred_element_type=F32
            )
            peaks[m, 0:1, :] = new
        return 0

    lax.fori_loop(0, chunks * rows // key_block, absorb, 0)
    if last:
        for m in range(2):
            acc = accs[m]
            total = acc[AV : AV + 1, :]
            send_ref[0, m * AV : (m + 1) * AV, :] = (acc[:AV] / total).astype(BF16)
            level = peaks[m, 0:1, :] + jnp.log(total)
            high = level.astype(BF16)
            left = level - high.astype(F32)
            middle = left.astype(BF16)
            low = (left - middle.astype(F32)).astype(BF16)
            at = 2 * AV + 8 * m
            send_ref[0, at : at + 8, :] = jnp.concatenate(
                [high.astype(F32), middle.astype(F32), low.astype(F32), jnp.zeros((5, width), F32)]
            ).astype(BF16)


def attend(queries, pieces, state=None, last=False):
    chunks, rows = len(pieces), pieces[0].shape[0]
    tiles = NX
    count = tiles * TOK
    first = state is None
    kv_spec = pl.BlockSpec((rows, 256), lambda i: (0, 0))
    q_spec = pl.BlockSpec((1, 2 * AK, TOK), lambda i: (i, 0, 0))
    peak_spec = pl.BlockSpec((2, 8, TOK), lambda i: (0, 0, i))
    acc_spec = pl.BlockSpec((2, ACC_ROWS, TOK), lambda i: (0, 0, i))
    state_specs = [peak_spec, acc_spec]
    state_shapes = [
        jax.ShapeDtypeStruct((2, 8, count), F32),
        jax.ShapeDtypeStruct((2, ACC_ROWS, count), F32),
    ]
    scratch = [pltpu.VMEM((chunks * rows, 128), BF16), pltpu.VMEM((ACC_ROWS, chunks * rows), BF16)]
    if first:
        in_specs = [pl.BlockSpec((TOK, 128), lambda i: (0, 0))] * NX + [kv_spec] * chunks
        operands = [*queries, *pieces]
    else:
        in_specs = [q_spec] + [kv_spec] * chunks + state_specs
        operands = [queries, *pieces, *state]
    if last:
        out_specs = [pl.BlockSpec((1, SEND_ROWS, TOK), lambda i: (i, 0, 0))]
        out_shape = [jax.ShapeDtypeStruct((tiles, SEND_ROWS, TOK), BF16)]
        scratch += [pltpu.VMEM((2, 8, TOK), F32), pltpu.VMEM((2, ACC_ROWS, TOK), F32)]
    else:
        out_specs, out_shape = state_specs, state_shapes
        if first:
            out_specs = [q_spec] + out_specs
            out_shape = [jax.ShapeDtypeStruct((tiles, 2 * AK, TOK), BF16)] + out_shape
    key_block = 1024 if chunks == 2 else TOK
    body = functools.partial(
        attend_body, first=first, last=last, chunks=chunks, key_block=key_block
    )
    work = 2 * count * chunks * rows
    return pl.pallas_call(
        body,
        grid=(tiles,),
        in_specs=in_specs,
        out_specs=out_specs,
        out_shape=out_shape,
        scratch_shapes=scratch,
        cost_estimate=cost(work * 2 * (AK + AV), work),
        compiler_params=pltpu.CompilerParams(vmem_limit_bytes=48 * 1024 * 1024),
        name="attend",
    )(*operands)


def mix_body(a_ref, b_ref, c_ref, d_ref, weight_ref, gain_ref, out_ref):
    refs = (a_ref, b_ref, c_ref, d_ref)
    mixed = None
    for m in range(2):
        at = 2 * AV + 8 * m
        levels = []
        for ref in refs:
            parts = ref[at : at + 8, :].astype(F32)
            levels.append(parts[0:1] + parts[1:2] + parts[2:3])
        peak = functools.reduce(jnp.maximum, levels)
        shares = [jnp.exp(level - peak) for level in levels]
        total = functools.reduce(jnp.add, shares)
        summed = None
        for ref, share in zip(refs, shares):
            term = ref[m * AV : (m + 1) * AV, :].astype(F32) * (share / total)
            summed = term if summed is None else summed + term
        mixed = summed if m == 0 else mixed - weight_ref[0] * summed
    scale = lax.rsqrt(jnp.mean(mixed * mixed, axis=0, keepdims=True) + EPS)
    out_ref[...] = ((mixed * scale).T * gain_ref[...]).astype(BF16)


def mix(partials, weight, gain):
    vmem = pl.BlockSpec(memory_space=pltpu.VMEM)
    return pl.pallas_call(
        mix_body,
        in_specs=[vmem] * 4 + [pl.BlockSpec(memory_space=pltpu.SMEM), vmem],
        out_specs=vmem,
        out_shape=jax.ShapeDtypeStruct((TOK, AV), BF16),
        name="mix",
    )(*partials, weight, gain.reshape(1, AV))


def on_device(
    tokens,
    norm_gain,
    rec_query,
    fwd_gate,
    bwd_gate,
    rec_value,
    gate_leak,
    log_decay,
    rec_gain,
    att_query,
    att_key,
    att_value,
    lambdas,
    att_gain,
    out_rec,
    out_att,
):
    z, x = lax.axis_index("z"), lax.axis_index("x")
    decays = jnp.broadcast_to(log_decay, (2, TOK, 128))
    cosine, sine = rotation_tables(TOK)
    weights_all = (att_key, att_value, att_query, rec_query, fwd_gate, bwd_gate, rec_value)
    joined = jnp.concatenate(weights_all, axis=1)
    normed = rms_scale(tokens.astype(F32), norm_gain).astype(BF16)
    projected = jnp.dot(gather_rows(normed), joined, preferred_element_type=F32).astype(BF16)
    own_kv = make_keys(projected, cosine, sine)
    ups, downs = [own_kv], [own_kv]
    for step in range(1, NZ // 2 + 1):
        ups.append(shift(ups[-1], "z", 1, NZ))
        if step < NZ // 2:
            downs.append(shift(downs[-1], "z", -1, NZ))
    pack, out_local, read_f, read_b = make_local(projected, gate_leak, decays, cosine, sine)
    packs = [pack]
    for by in (1, 2, -1):
        packs.append(shift(pack, "x", by, NX))
    kept, sent = fold_x(x.reshape(1), packs)
    turned, *state = attend([packs[0], packs[1], packs[3], packs[2]], [own_kv])
    for bit in (1, 2, 4):
        received = lax.ppermute(sent, "z", [(i, i ^ bit) for i in range(NZ)])
        lower = ((z // bit) % 2).astype(jnp.int32).reshape(1)
        if bit < 4:
            kept, sent = merge(lower, kept, received)
    state = attend(turned, [ups[1], downs[1]], state)
    state = attend(turned, [ups[2], downs[2]], state)
    sends = attend(turned, [ups[3], downs[3], ups[4]], state, last=True)[0]
    half = SEND_ROWS // 2
    far_low = shift(sends[3, :half], "x", 2, NX)
    far_high = shift(sends[3, half:], "x", -2, NX)
    from_above = shift(sends[1], "x", -1, NX)
    from_below = shift(sends[2], "x", 1, NX)
    rec_rows = finish(lower, kept, received, out_local, read_f, read_b, rec_gain)
    rec_all = lax.all_to_all(rec_rows, TP, split_axis=0, concat_axis=1, tiled=True)
    rec_part = jnp.dot(rec_all, out_rec, preferred_element_type=F32)
    far = jnp.concatenate([far_low, far_high])
    att_rows = mix([sends[0], from_above, from_below, far], lambdas, att_gain)
    att_all = lax.all_to_all(att_rows, TP, split_axis=0, concat_axis=1, tiled=True)
    return (rec_part + jnp.dot(att_all, out_att, preferred_element_type=F32)).astype(BF16)


def solution(mesh):
    torus = Mesh(mesh.devices.reshape(NZ, NX, NY, NC), AXES)
    in_specs = (
        P(AXES, None),
        P(),
        P(None, TP),
        P(None, TP),
        P(None, TP),
        P(None, TP),
        P(None, TP),
        P(None, SP, TP),
        P(),
        P(None, TP),
        P(None, TP),
        P(None, TP),
        P(TP),
        P(),
        P(),
        P(),
    )
    out_specs = P(AXES, None)
    return jax.shard_map(
        on_device, mesh=torus, in_specs=in_specs, out_specs=out_specs, check_vma=False
    )
```

```python
import functools

import jax
import jax.numpy as jnp
from jax import lax
from jax.experimental import pallas as pl
from jax.experimental.pallas import tpu as pltpu
from jax.sharding import Mesh
from jax.sharding import PartitionSpec as P


HK = 128
HV = 128
AK = 64
AV = 128
BLOCK = 64
NZ, NX, NY, NC = 8, 4, 4, 2
AXES = ("z", "x", "y", "c")
SP = ("z", "x")
TP = ("y", "c")
TOK = 512
ACC_ROWS = 144
MAP_ROWS = AV + 16
SEND_ROWS = 2 * MAP_ROWS
PACK = 784
BF16 = jnp.bfloat16
F32 = jnp.float32

EPS = 1e-06
THETA = 500000.0
RISE = 40.0


def shift(value, axis, by, size):
    return lax.ppermute(value, axis, [(i, (i + by) % size) for i in range(size)])


def gather_rows(rows):
    half = rows.shape[0] // 2
    far_low = shift(rows[:half], "y", 2, NY)
    far_high = shift(rows[half:], "y", -2, NY)
    up = shift(rows, "y", 1, NY)
    down = shift(rows, "y", -1, NY)
    mine = jnp.concatenate([rows, up, down, far_low, far_high])
    return mine, shift(mine, "c", 1, NC)


def rms_scale(values, gain):
    return values * lax.rsqrt(jnp.mean(values * values, axis=-1, keepdims=True) + EPS) * gain


VMEM = pl.BlockSpec(memory_space=pltpu.VMEM)
SMEM = pl.BlockSpec(memory_space=pltpu.SMEM)


def limit(mib):
    return pltpu.CompilerParams(vmem_limit_bytes=mib << 20)


def cost(flops, transcendentals=0):
    return pl.CostEstimate(flops=flops, transcendentals=transcendentals, bytes_accessed=1 << 20)


def rotation_tables(length):
    positions = (lax.axis_index(SP) * length + jnp.arange(length, dtype=jnp.int32)).astype(F32)
    frequency = THETA ** (-(jnp.arange(AK // 2, dtype=F32) * 2.0 / AK))
    angles = positions[:, None] * frequency[None, :]
    cosine, sine = jnp.cos(angles), jnp.sin(angles)
    return (
        jnp.concatenate([cosine] * 4, axis=1),
        jnp.concatenate([-sine, sine, -sine, sine], axis=1),
    )


def rotated(vectors, cosine, sine):
    lane = lax.broadcasted_iota(jnp.int32, vectors.shape, 1)
    half = AK // 2
    partner = jnp.where(
        (lane & half) == 0, pltpu.roll(vectors, 128 - half, 1), pltpu.roll(vectors, half, 1)
    )
    return vectors * cosine + partner * sine


def keys_body(
    place_ref, mine_ref, other_ref, key_ref, value_ref, cos_ref, sin_ref, rows_ref, out_ref
):
    y, c = place_ref[2], place_ref[3]
    size = mine_ref.shape[0] // NY
    for core, ref in ((c, mine_ref), (1 - c, other_ref)):
        for n, distance in enumerate((0, 3, 1, 2)):
            at = pl.multiple_of((((y + distance) % NY) * NC + core) * size, size)
            rows_ref[pl.ds(at, size), :] = ref[n * size : (n + 1) * size, :]
    weights = jnp.concatenate([key_ref[...], value_ref[...]], axis=1)
    raw = jnp.dot(rows_ref[...], weights, preferred_element_type=F32).astype(BF16)
    out_ref[:TOK, :] = rotated(raw[:, :128].astype(F32), cos_ref[...], sin_ref[...]).astype(BF16)
    for n in range(TOK // 128):
        out_ref[TOK + n * 128 : TOK + (n + 1) * 128, :] = raw[n * 128 : (n + 1) * 128, 128:].T


def make_keys(place, mine, other, key, value, cosine, sine):
    return pl.pallas_call(
        keys_body,
        in_specs=[SMEM] + [VMEM] * 6,
        out_specs=[VMEM, VMEM],
        out_shape=[
            jax.ShapeDtypeStruct((TOK, mine.shape[1]), BF16),
            jax.ShapeDtypeStruct((2 * TOK, 128), BF16),
        ],
        cost_estimate=cost(1 << 29),
        compiler_params=limit(6),
        name="make_keys",
    )(place, mine, other, key, value, cosine, sine)


def local_body(
    rows_ref, aq_ref, q_ref, f_ref, b_ref, v_ref, leak_ref, decay_ref, cos_ref, sin_ref,
    pack_ref, out_ref, read_f_ref, read_b_ref,
):
    def project(*weights):
        joined = jnp.concatenate([w[...] for w in weights], axis=1)
        return jnp.dot(rows_ref[...], joined, preferred_element_type=F32).astype(BF16)

    raw_f_b = project(f_ref, b_ref)
    raw_q_v = project(q_ref, v_ref)
    raw_aq = project(aq_ref)
    pack_ref[:TOK, :] = (
        rotated(raw_aq.astype(F32), cos_ref[...], sin_ref[...]) * AK ** (-0.5)
    ).astype(BF16)
    raw = raw_q_v[:, :128].astype(F32)
    queries = raw / (1.0 + jnp.exp(-raw))
    row = lax.broadcasted_iota(jnp.int32, (BLOCK, BLOCK), 0)
    col = lax.broadcasted_iota(jnp.int32, (BLOCK, BLOCK), 1)
    totals = []
    for way, read_ref in enumerate((read_f_ref, read_b_ref)):
        gates = raw_f_b[:, way * HK : (way + 1) * HK].astype(F32)
        keys = leak_ref[way : way + 1, :] / (1.0 + jnp.exp(gates))
        logs = jnp.log1p(-keys) + decay_ref[way]
        reach = (row >= col) if way == 0 else (row <= col)
        sums = jnp.where(reach, 1.0, 0.0)
        middle_row, last_row = (BLOCK // 2 - 1, BLOCK - 1) if way == 0 else (BLOCK // 2, 0)
        state = jnp.zeros((HV, HK), F32)
        before = jnp.zeros((1, HK), F32)
        blocks = range(TOK // BLOCK)
        for n in blocks if way == 0 else reversed(blocks):
            at = slice(n * BLOCK, (n + 1) * BLOCK)
            cumulative = jnp.dot(
                sums, logs[at], precision=lax.Precision.HIGHEST, preferred_element_type=F32
            )
            middle = cumulative[middle_row : middle_row + 1]
            last = cumulative[last_row : last_row + 1]
            scores = lax.dot_general(
                (queries[at] * jnp.exp(cumulative - middle)).astype(BF16),
                (keys[at] * jnp.exp(middle - cumulative)).astype(BF16),
                (((1,), (1,)), ((), ())),
                preferred_element_type=F32,
            )
            scores = jnp.where(reach, scores, 0.0).astype(BF16)
            values = raw_q_v[at, 128:]
            out = jnp.dot(scores, values, preferred_element_type=F32)
            read = queries[at] * jnp.exp(cumulative)
            out = out + lax.dot_general(
                read.astype(BF16),
                state.astype(BF16),
                (((1,), (1,)), ((), ())),
                preferred_element_type=F32,
            )
            out_ref[at, :] = out if way == 0 else out_ref[at, :] + out
            read_ref[at, :] = (read * jnp.exp(before)).astype(BF16)
            added = lax.dot_general(
                values,
                (keys[at] * jnp.exp(last - cumulative)).astype(BF16),
                (((0,), (0,)), ((), ())),
                preferred_element_type=F32,
            )
            state = state * jnp.exp(last) + added
            before = before + last
        pack_ref[TOK + way * HV : TOK + (way + 1) * HV, :] = state.astype(BF16)
        totals.append(jnp.exp(before))
    pack_ref[TOK + 2 * HV :, :] = jnp.concatenate(
        [*totals, jnp.zeros((PACK - TOK - 2 * HV - 2, HK), F32)]
    ).astype(BF16)


def make_local(rows, weights, leak, decays, cosine, sine):
    return pl.pallas_call(
        local_body,
        in_specs=[VMEM] * 10,
        out_specs=[VMEM] * 4,
        out_shape=[
            jax.ShapeDtypeStruct((PACK, 128), BF16),
            jax.ShapeDtypeStruct((TOK, 128), F32),
            jax.ShapeDtypeStruct((TOK, 128), BF16),
            jax.ShapeDtypeStruct((TOK, 128), BF16),
        ],
        cost_estimate=cost(1 << 31),
        compiler_params=limit(12),
        name="local",
    )(rows, *weights, leak, decays, cosine, sine)


def link(earlier, later):
    return (earlier[0] * later[0], later[0] * earlier[1] + later[1])


def pick(condition, new, old):
    return tuple(jnp.where(condition, a, b) for a, b in zip(new, old))


def read_sent(ref, at):
    decays = ref[at + 2 * HV : at + 2 * HV + 16, :].astype(F32)
    return (
        (decays[0:1], ref[at : at + HV, :].astype(F32)),
        (decays[1:2], ref[at + HV : at + 2 * HV, :].astype(F32)),
    )


def write_sent(ref, fwd, bwd):
    ref[:HV, :] = fwd[1].astype(BF16)
    ref[HV : 2 * HV, :] = bwd[1].astype(BF16)
    ref[2 * HV :, :] = jnp.concatenate([fwd[0], bwd[0], jnp.zeros((14, HK), F32)]).astype(BF16)


def write_kept(ref, n, pair):
    ref[n, :HV, :] = pair[1]
    ref[n, HV:, :] = jnp.broadcast_to(pair[0], (8, HK))


def read_kept(ref, n):
    return ref[n, HV : HV + 1, :], ref[n, :HV, :]


def fold_body(place_ref, own_ref, below1_ref, below2_ref, below3_ref, kept_ref, sent_ref):
    place = place_ref[1]
    entries = [read_sent(ref, TOK) for ref in (own_ref, below1_ref, below2_ref, below3_ref)]
    none = (jnp.ones((1, HK), F32), jnp.zeros((HV, HK), F32))

    def fold(way, below, order):
        found = none
        for k in order:
            passed = (place >= k) if below else (place < k)
            found = pick(passed, link(found, entries[k][way]), found)
        return found

    f_below, f_above = fold(0, True, (3, 2, 1)), fold(0, False, (3, 2, 1))
    b_above, b_below = fold(1, False, (1, 2, 3)), fold(1, True, (1, 2, 3))
    fwd = link(link(f_below, entries[0][0]), f_above)
    bwd = link(link(b_above, entries[0][1]), b_below)
    for n, pair in enumerate((fwd, bwd, f_below, b_above)):
        write_kept(kept_ref, n, pair)
    write_sent(sent_ref, fwd, bwd)


KEPT = jax.ShapeDtypeStruct((4, HV + 8, HK), F32)
SENT = jax.ShapeDtypeStruct((2 * HV + 16, HK), BF16)


def fold_x(place, packs):
    return pl.pallas_call(
        fold_body,
        in_specs=[SMEM] + [VMEM] * 4,
        out_specs=[VMEM, VMEM],
        out_shape=[KEPT, SENT],
        cost_estimate=cost(1 << 22),
        compiler_params=limit(4),
        name="fold_x",
    )(place, *packs)


def is_lower(place_ref, bit):
    return (place_ref[0] & bit) != 0


def met(lower, kept_ref, received_ref):
    fwd, bwd, before, after = (read_kept(kept_ref, n) for n in range(4))
    peer_f, peer_b = read_sent(received_ref, 0)
    return (
        pick(lower, link(peer_f, fwd), link(fwd, peer_f)),
        pick(lower, link(bwd, peer_b), link(peer_b, bwd)),
        pick(lower, link(peer_f, before), before),
        pick(lower, after, link(peer_b, after)),
    )


def merge_body(place_ref, kept_ref, received_ref, out_ref, sent_ref, *, bit):
    pairs = met(is_lower(place_ref, bit), kept_ref, received_ref)
    for n, pair in enumerate(pairs):
        write_kept(out_ref, n, pair)
    write_sent(sent_ref, pairs[0], pairs[1])


def merge(place, bit, kept, received):
    return pl.pallas_call(
        functools.partial(merge_body, bit=bit),
        in_specs=[SMEM, VMEM, VMEM],
        out_specs=[VMEM, VMEM],
        out_shape=[KEPT, SENT],
        cost_estimate=cost(1 << 22),
        compiler_params=limit(4),
        name="merge",
    )(place, kept, received)


def finish_body(
    place_ref, kept_ref, received_ref, out_ref, read_f_ref, read_b_ref, gain_ref, rows_ref, *, bit
):
    _, _, before, after = met(is_lower(place_ref, bit), kept_ref, received_ref)
    total = out_ref[...]
    for read_ref, (_, state) in ((read_f_ref, before), (read_b_ref, after)):
        total = total + lax.dot_general(
            read_ref[...], state.astype(BF16), (((1,), (1,)), ((), ())), preferred_element_type=F32
        )
    rows_ref[...] = rms_scale(total, gain_ref[...]).astype(BF16)


def finish(place, bit, kept, received, out, read_f, read_b, gain):
    return pl.pallas_call(
        functools.partial(finish_body, bit=bit),
        in_specs=[SMEM] + [VMEM] * 6,
        out_specs=VMEM,
        out_shape=jax.ShapeDtypeStruct((TOK, HV), BF16),
        cost_estimate=cost(1 << 25),
        compiler_params=limit(4),
        name="finish",
    )(place, kept, received, out, read_f, read_b, gain.reshape(1, HV))


def attend_tile(maps, kv_refs, peaks, accs, first):
    ones = jnp.ones((ACC_ROWS - AV, TOK), BF16)
    values = [
        jnp.concatenate(
            [
                jnp.concatenate(
                    [kv[TOK + n * 128 : TOK + (n + 1) * 128, :] for n in range(TOK // 128)], axis=1
                ),
                ones,
            ]
        )
        for kv in kv_refs
    ]
    accs, peaks, rises = list(accs), list(peaks), []
    units = [(m, n) for m in range(len(maps)) for n in range(len(kv_refs))]

    def scores_of(unit):
        return jnp.dot(kv_refs[unit[1]][:TOK, :], maps[unit[0]], preferred_element_type=F32)

    scores = scores_of(units[0])
    for at, (m, n) in enumerate(units):
        upcoming = scores_of(units[at + 1]) if at + 1 < len(units) else None
        if first:
            peaks[m] = jnp.max(scores, axis=0, keepdims=True)
        above = scores - peaks[m]
        if not first:
            rises.append(jnp.max(above.reshape(-1, 8, above.shape[1]), axis=0))
        added = jnp.dot(values[n], jnp.exp(above).astype(BF16), preferred_element_type=F32)
        accs[m] = added if first else accs[m] + added
        scores = upcoming
    return accs, peaks, None if first else jnp.max(functools.reduce(jnp.maximum, rises))


def attend_again(maps_ref, kv_refs, peaks_ref, accs_ref):
    ones = jnp.ones((ACC_ROWS - AV, 128), BF16)
    for kv in kv_refs:

        def absorb(i, unused):
            m, n = i // (TOK // 128), i % (TOK // 128)
            keys = kv[pl.ds(pl.multiple_of(n * 128, 128), 128), :]
            values = kv[pl.ds(pl.multiple_of(TOK + n * 128, 128), 128), :]
            scores = jnp.dot(keys, maps_ref[m], preferred_element_type=F32)
            old = peaks_ref[m, 0:1, :]
            new = jnp.maximum(old, jnp.max(scores, axis=0, keepdims=True))
            accs_ref[m] = accs_ref[m] * jnp.exp(old - new) + jnp.dot(
                jnp.concatenate([values, ones]),
                jnp.exp(scores - new).astype(BF16),
                preferred_element_type=F32,
            )
            peaks_ref[m, 0:1, :] = new
            return 0

        lax.fori_loop(0, 2 * TOK // 128, absorb, 0)


def both_maps(turned):
    upper = lax.broadcasted_iota(jnp.int32, turned.shape, 0) < AK
    zero = jnp.zeros_like(turned)
    return jnp.where(upper, turned, zero), jnp.where(upper, zero, turned)


def attend_first_body(*refs):
    q_refs, (kv_ref, turned_ref, peaks_ref, accs_ref) = refs[:NX], refs[NX:]
    for n, ref in enumerate(q_refs):
        turned_ref[n] = ref[:TOK, :].T

    def tile(t, unused):
        accs, peaks, _ = attend_tile(
            both_maps(turned_ref[t]), [kv_ref], [None] * 2, [None] * 2, True
        )
        for m in range(2):
            accs_ref[t, m] = accs[m]
            peaks_ref[t, m] = jnp.broadcast_to(peaks[m], (8, TOK))
        return 0

    lax.fori_loop(0, NX, tile, 0)


def attend_more_body(turned_ref, *refs, chunks):
    kv_refs, (peaks_in, accs_in, peaks_ref, accs_ref, maps_ref) = refs[:chunks], refs[chunks:]
    peaks_ref[...] = peaks_in[...]

    def tile(t, unused):
        maps = both_maps(turned_ref[t])
        peaks = [peaks_in[t, m, 0:1, :] for m in range(2)]
        accs, _, rise = attend_tile(maps, kv_refs, peaks, [accs_in[t, m] for m in range(2)], False)
        for m in range(2):
            accs_ref[t, m] = accs[m]

        @pl.when(rise > RISE)
        def _():
            maps_ref[0], maps_ref[1] = maps
            accs_ref[t] = accs_in[t]
            attend_again(maps_ref, kv_refs, peaks_ref.at[t], accs_ref.at[t])

        return 0

    lax.fori_loop(0, NX, tile, 0)


def attend_last_body(turned_ref, *refs, chunks, tile):
    kv_refs, rest = refs[:chunks], refs[chunks:]
    peaks_in, accs_in, *send_refs, peaks_ref, accs_ref, maps_ref, rise_ref = rest
    maps_ref[0], maps_ref[1] = both_maps(turned_ref[tile])
    peaks_ref[...] = peaks_in[tile]
    rise_ref[0] = 0.0

    def one_map(m, unused):
        accs, _, rise = attend_tile(
            [maps_ref[m]], kv_refs, [peaks_in[tile, m, 0:1, :]], [accs_in[tile, m]], False
        )
        accs_ref[m] = accs[0]
        rise_ref[0] = jnp.maximum(rise_ref[0], rise)
        return 0

    lax.fori_loop(0, 2, one_map, 0)

    @pl.when(rise_ref[0] > RISE)
    def _():
        accs_ref[...] = accs_in[tile]
        attend_again(maps_ref, kv_refs, peaks_ref, accs_ref)

    for m in range(2):
        acc = accs_ref[m]
        total = acc[AV : AV + 1, :]
        level = peaks_ref[m, 0:1, :] + jnp.log(total)
        high = level.astype(BF16)
        left = level - high.astype(F32)
        middle = left.astype(BF16)
        low = (left - middle.astype(F32)).astype(BF16)
        mean = (acc[:AV] * (1.0 / total)).astype(BF16)
        levels = jnp.concatenate(
            [high.astype(F32), middle.astype(F32), low.astype(F32), jnp.zeros((13, TOK), F32)]
        ).astype(BF16)
        ref = send_refs[m] if len(send_refs) > 1 else send_refs[0]
        at = 0 if len(send_refs) > 1 else m * MAP_ROWS
        ref[at : at + AV, :] = mean
        ref[at + AV : at + MAP_ROWS, :] = levels


STATE = [
    jax.ShapeDtypeStruct((NX, 2, 8, TOK), F32),
    jax.ShapeDtypeStruct((NX, 2, ACC_ROWS, TOK), F32),
]


def attend_cost(tiles, chunks):
    work = 2 * tiles * TOK * chunks * TOK
    return cost(work * 2 * (AK + AV), work)


def attend_first(packs, kv):
    return pl.pallas_call(
        attend_first_body,
        in_specs=[VMEM] * (NX + 1),
        out_specs=[VMEM] * 3,
        out_shape=[jax.ShapeDtypeStruct((NX, 2 * AK, TOK), BF16), *STATE],
        cost_estimate=attend_cost(NX, 1),
        compiler_params=limit(14),
        name="attend_first",
    )(*packs, kv)


def attend_more(turned, pieces, state):
    return pl.pallas_call(
        functools.partial(attend_more_body, chunks=len(pieces)),
        in_specs=[VMEM] * (len(pieces) + 3),
        out_specs=[VMEM] * 2,
        out_shape=STATE,
        scratch_shapes=[pltpu.VMEM((2, 2 * AK, TOK), BF16)],
        cost_estimate=attend_cost(NX, len(pieces)),
        compiler_params=limit(14),
        name="attend_more",
    )(turned, *pieces, *state)


def attend_last(turned, pieces, state, tile, parts):
    return pl.pallas_call(
        functools.partial(attend_last_body, chunks=len(pieces), tile=tile),
        in_specs=[VMEM] * (len(pieces) + 3),
        out_specs=[VMEM] * parts,
        out_shape=[jax.ShapeDtypeStruct((SEND_ROWS // parts, TOK), BF16)] * parts,
        scratch_shapes=[
            pltpu.VMEM((2, 8, TOK), F32),
            pltpu.VMEM((2, ACC_ROWS, TOK), F32),
            pltpu.VMEM((2, 2 * AK, TOK), BF16),
            pltpu.SMEM((1,), F32),
        ],
        cost_estimate=attend_cost(1, len(pieces)),
        compiler_params=limit(14),
        name="attend_last",
    )(turned, *pieces, *state)


def mix_body(a_ref, b_ref, c_ref, low_ref, high_ref, weight_ref, gain_ref, out_ref):
    mixed = None
    for m in range(2):
        places = [(ref, m * MAP_ROWS) for ref in (a_ref, b_ref, c_ref)]
        places.append(((low_ref, high_ref)[m], 0))
        levels = []
        for ref, at in places:
            parts = ref[at + AV : at + MAP_ROWS, :].astype(F32)
            levels.append(parts[0:1] + parts[1:2] + parts[2:3])
        peak = functools.reduce(jnp.maximum, levels)
        shares = [jnp.exp(level - peak) for level in levels]
        scale = 1.0 / functools.reduce(jnp.add, shares)
        if m == 1:
            scale = scale * -weight_ref[0]
        for (ref, at), share in zip(places, shares):
            term = ref[at : at + AV, :].astype(F32) * (share * scale)
            mixed = term if mixed is None else mixed + term
    scale = lax.rsqrt(jnp.mean(mixed * mixed, axis=0, keepdims=True) + EPS)
    out_ref[...] = ((mixed * scale).T * gain_ref[...]).astype(BF16)


def mix(partials, weight, gain):
    return pl.pallas_call(
        mix_body,
        in_specs=[VMEM] * 5 + [SMEM, VMEM],
        out_specs=VMEM,
        out_shape=jax.ShapeDtypeStruct((TOK, AV), BF16),
        cost_estimate=cost(1 << 22),
        compiler_params=limit(6),
        name="mix",
    )(*partials, weight, gain.reshape(1, AV))


def on_device(
    tokens,
    norm_gain,
    rec_query,
    fwd_gate,
    bwd_gate,
    rec_value,
    gate_leak,
    log_decay,
    rec_gain,
    att_query,
    att_key,
    att_value,
    lambdas,
    att_gain,
    out_rec,
    out_att,
):
    place = jnp.stack([lax.axis_index(axis) for axis in AXES]).astype(jnp.int32)
    decays = jnp.broadcast_to(log_decay, (2, TOK, 128))
    cosine, sine = rotation_tables(TOK)
    normed = rms_scale(tokens.astype(F32), norm_gain).astype(BF16)
    mine, other = gather_rows(normed)
    rows, own_kv = make_keys(place, mine, other, att_key, att_value, cosine, sine)
    ups, downs = [own_kv], [own_kv]
    for step in range(1, NZ // 2 + 1):
        ups.append(shift(ups[-1], "z", 1, NZ))
        if step < NZ // 2:
            downs.append(shift(downs[-1], "z", -1, NZ))
    pack, out_local, read_f, read_b = make_local(
        rows,
        (att_query, rec_query, fwd_gate, bwd_gate, rec_value),
        gate_leak,
        decays,
        cosine,
        sine,
    )
    packs = [pack]
    for by in (1, 2, -1):
        packs.append(shift(pack, "x", by, NX))
    kept, sent = fold_x(place, packs)
    turned, *state = attend_first([packs[0], packs[1], packs[3], packs[2]], own_kv)
    for bit in (1, 2, 4):
        received = lax.ppermute(sent, "z", [(i, i ^ bit) for i in range(NZ)])
        if bit < 4:
            kept, sent = merge(place, bit, kept, received)
    state = attend_more(turned, [ups[1], downs[1]], state)
    state = attend_more(turned, [ups[2], downs[2]], state)
    ends = [ups[3], downs[3], ups[4]]
    low, high = attend_last(turned, ends, state, 3, 2)
    far_low = shift(low, "x", 2, NX)
    far_high = shift(high, "x", -2, NX)
    (send,) = attend_last(turned, ends, state, 1, 1)
    from_above = shift(send, "x", -1, NX)
    (send,) = attend_last(turned, ends, state, 2, 1)
    from_below = shift(send, "x", 1, NX)
    (own,) = attend_last(turned, ends, state, 0, 1)
    rec_rows = finish(place, bit, kept, received, out_local, read_f, read_b, rec_gain)
    rec_all = lax.all_to_all(rec_rows, TP, split_axis=0, concat_axis=1, tiled=True)
    rec_part = jnp.dot(rec_all, out_rec, preferred_element_type=F32)
    att_rows = mix([own, from_above, from_below, far_low, far_high], lambdas, att_gain)
    att_all = lax.all_to_all(att_rows, TP, split_axis=0, concat_axis=1, tiled=True)
    return (rec_part + jnp.dot(att_all, out_att, preferred_element_type=F32)).astype(BF16)


def solution(mesh):
    torus = Mesh(mesh.devices.reshape(NZ, NX, NY, NC), AXES)
    in_specs = (
        P(AXES, None),
        P(),
        P(None, TP),
        P(None, TP),
        P(None, TP),
        P(None, TP),
        P(None, TP),
        P(None, SP, TP),
        P(),
        P(None, TP),
        P(None, TP),
        P(None, TP),
        P(TP),
        P(),
        P(),
        P(),
    )
    out_specs = P(AXES, None)
    return jax.shard_map(
        on_device, mesh=torus, in_specs=in_specs, out_specs=out_specs, check_vma=False
    )
```

```python
import functools

import jax
import jax.numpy as jnp
from jax import lax
from jax.experimental import pallas as pl
from jax.experimental.pallas import tpu as pltpu
from jax.sharding import Mesh
from jax.sharding import PartitionSpec as P


HK = 128
HV = 128
AK = 64
AV = 128
BLOCK = 64
NZ, NX, NY, NC = 8, 4, 4, 2
AXES = ("z", "x", "y", "c")
SP = ("z", "x")
TP = ("y", "c")
TOK = 512
ACC_ROWS = 144
MAP_ROWS = AV + 16
SEND_ROWS = 2 * MAP_ROWS
PACK = 784
BF16 = jnp.bfloat16
F32 = jnp.float32

EPS = 1e-06
THETA = 500000.0
RISE = 40.0


def shift(value, axis, by, size):
    return lax.ppermute(value, axis, [(i, (i + by) % size) for i in range(size)])


def gather_rows(rows):
    half = rows.shape[0] // 2
    far_low = shift(rows[:half], "y", 2, NY)
    far_high = shift(rows[half:], "y", -2, NY)
    up = shift(rows, "y", 1, NY)
    down = shift(rows, "y", -1, NY)
    mine = jnp.concatenate([rows, up, down, far_low, far_high])
    return mine, shift(mine, "c", 1, NC)


def rms_scale(values, gain):
    return values * lax.rsqrt(jnp.mean(values * values, axis=-1, keepdims=True) + EPS) * gain


VMEM = pl.BlockSpec(memory_space=pltpu.VMEM)
SMEM = pl.BlockSpec(memory_space=pltpu.SMEM)


def limit(mib):
    return pltpu.CompilerParams(vmem_limit_bytes=mib << 20)


def cost(flops, transcendentals=0):
    return pl.CostEstimate(flops=flops, transcendentals=transcendentals, bytes_accessed=1 << 20)


def rotation_tables(length):
    positions = (lax.axis_index(SP) * length + jnp.arange(length, dtype=jnp.int32)).astype(F32)
    frequency = THETA ** (-(jnp.arange(AK // 2, dtype=F32) * 2.0 / AK))
    angles = positions[:, None] * frequency[None, :]
    cosine, sine = jnp.cos(angles), jnp.sin(angles)
    return (
        jnp.concatenate([cosine] * 4, axis=1),
        jnp.concatenate([-sine, sine, -sine, sine], axis=1),
    )


def rotated(vectors, cosine, sine):
    lane = lax.broadcasted_iota(jnp.int32, vectors.shape, 1)
    half = AK // 2
    partner = jnp.where(
        (lane & half) == 0, pltpu.roll(vectors, 128 - half, 1), pltpu.roll(vectors, half, 1)
    )
    return vectors * cosine + partner * sine


def keys_body(
    place_ref, mine_ref, other_ref, key_ref, value_ref, cos_ref, sin_ref, rows_ref, out_ref
):
    y, c = place_ref[2], place_ref[3]
    size = mine_ref.shape[0] // NY
    for core, ref in ((c, mine_ref), (1 - c, other_ref)):
        for n, distance in enumerate((0, 3, 1, 2)):
            at = pl.multiple_of((((y + distance) % NY) * NC + core) * size, size)
            rows_ref[pl.ds(at, size), :] = ref[n * size : (n + 1) * size, :]
    weights = jnp.concatenate([key_ref[...], value_ref[...]], axis=1)
    raw = jnp.dot(rows_ref[...], weights, preferred_element_type=F32).astype(BF16)
    out_ref[:TOK, :] = rotated(raw[:, :128].astype(F32), cos_ref[...], sin_ref[...]).astype(BF16)
    for n in range(TOK // 128):
        out_ref[TOK + n * 128 : TOK + (n + 1) * 128, :] = raw[n * 128 : (n + 1) * 128, 128:].T


def make_keys(place, mine, other, key, value, cosine, sine):
    return pl.pallas_call(
        keys_body,
        in_specs=[SMEM] + [VMEM] * 6,
        out_specs=[VMEM, VMEM],
        out_shape=[
            jax.ShapeDtypeStruct((TOK, mine.shape[1]), BF16),
            jax.ShapeDtypeStruct((2 * TOK, 128), BF16),
        ],
        cost_estimate=cost(1 << 29),
        compiler_params=limit(6),
        name="make_keys",
    )(place, mine, other, key, value, cosine, sine)


def local_body(
    rows_ref, aq_ref, q_ref, f_ref, b_ref, v_ref, leak_ref, decay_ref, cos_ref, sin_ref,
    pack_ref, out_ref, read_f_ref, read_b_ref,
):
    def project(*weights):
        joined = jnp.concatenate([w[...] for w in weights], axis=1)
        return jnp.dot(rows_ref[...], joined, preferred_element_type=F32).astype(BF16)

    raw_f_b = project(f_ref, b_ref)
    raw_q_v = project(q_ref, v_ref)
    raw_aq = project(aq_ref)
    pack_ref[:TOK, :] = (
        rotated(raw_aq.astype(F32), cos_ref[...], sin_ref[...]) * AK ** (-0.5)
    ).astype(BF16)
    raw = raw_q_v[:, :128].astype(F32)
    queries = raw / (1.0 + jnp.exp(-raw))
    row = lax.broadcasted_iota(jnp.int32, (BLOCK, BLOCK), 0)
    col = lax.broadcasted_iota(jnp.int32, (BLOCK, BLOCK), 1)
    totals = []
    for way, read_ref in enumerate((read_f_ref, read_b_ref)):
        gates = raw_f_b[:, way * HK : (way + 1) * HK].astype(F32)
        keys = leak_ref[way : way + 1, :] / (1.0 + jnp.exp(gates))
        logs = jnp.log1p(-keys) + decay_ref[way]
        reach = (row >= col) if way == 0 else (row <= col)
        sums = jnp.where(reach, 1.0, 0.0)
        middle_row, last_row = (BLOCK // 2 - 1, BLOCK - 1) if way == 0 else (BLOCK // 2, 0)
        state = jnp.zeros((HV, HK), F32)
        before = jnp.zeros((1, HK), F32)
        blocks = range(TOK // BLOCK)
        for n in blocks if way == 0 else reversed(blocks):
            at = slice(n * BLOCK, (n + 1) * BLOCK)
            cumulative = jnp.dot(
                sums, logs[at], precision=lax.Precision.HIGHEST, preferred_element_type=F32
            )
            middle = cumulative[middle_row : middle_row + 1]
            last = cumulative[last_row : last_row + 1]
            scores = lax.dot_general(
                (queries[at] * jnp.exp(cumulative - middle)).astype(BF16),
                (keys[at] * jnp.exp(middle - cumulative)).astype(BF16),
                (((1,), (1,)), ((), ())),
                preferred_element_type=F32,
            )
            scores = jnp.where(reach, scores, 0.0).astype(BF16)
            values = raw_q_v[at, 128:]
            out = jnp.dot(scores, values, preferred_element_type=F32)
            read = queries[at] * jnp.exp(cumulative)
            out = out + lax.dot_general(
                read.astype(BF16),
                state.astype(BF16),
                (((1,), (1,)), ((), ())),
                preferred_element_type=F32,
            )
            out_ref[at, :] = out if way == 0 else out_ref[at, :] + out
            read_ref[at, :] = (read * jnp.exp(before)).astype(BF16)
            added = lax.dot_general(
                values,
                (keys[at] * jnp.exp(last - cumulative)).astype(BF16),
                (((0,), (0,)), ((), ())),
                preferred_element_type=F32,
            )
            state = state * jnp.exp(last) + added
            before = before + last
        pack_ref[TOK + way * HV : TOK + (way + 1) * HV, :] = state.astype(BF16)
        totals.append(jnp.exp(before))
    pack_ref[TOK + 2 * HV :, :] = jnp.concatenate(
        [*totals, jnp.zeros((PACK - TOK - 2 * HV - 2, HK), F32)]
    ).astype(BF16)


def make_local(rows, weights, leak, decays, cosine, sine):
    return pl.pallas_call(
        local_body,
        in_specs=[VMEM] * 10,
        out_specs=[VMEM] * 4,
        out_shape=[
            jax.ShapeDtypeStruct((PACK, 128), BF16),
            jax.ShapeDtypeStruct((TOK, 128), F32),
            jax.ShapeDtypeStruct((TOK, 128), BF16),
            jax.ShapeDtypeStruct((TOK, 128), BF16),
        ],
        cost_estimate=cost(1 << 31),
        compiler_params=limit(12),
        name="local",
    )(rows, *weights, leak, decays, cosine, sine)


def link(earlier, later):
    return (earlier[0] * later[0], later[0] * earlier[1] + later[1])


def pick(condition, new, old):
    return tuple(jnp.where(condition, a, b) for a, b in zip(new, old))


def read_sent(ref, at):
    decays = ref[at + 2 * HV : at + 2 * HV + 16, :].astype(F32)
    return (
        (decays[0:1], ref[at : at + HV, :].astype(F32)),
        (decays[1:2], ref[at + HV : at + 2 * HV, :].astype(F32)),
    )


def write_sent(ref, fwd, bwd):
    ref[:HV, :] = fwd[1].astype(BF16)
    ref[HV : 2 * HV, :] = bwd[1].astype(BF16)
    ref[2 * HV :, :] = jnp.concatenate([fwd[0], bwd[0], jnp.zeros((14, HK), F32)]).astype(BF16)


def write_kept(ref, n, pair):
    ref[n, :HV, :] = pair[1]
    ref[n, HV:, :] = jnp.broadcast_to(pair[0], (8, HK))


def read_kept(ref, n):
    return ref[n, HV : HV + 1, :], ref[n, :HV, :]


def fold_body(place_ref, own_ref, below1_ref, below2_ref, below3_ref, kept_ref, sent_ref):
    place = place_ref[1]
    entries = [read_sent(ref, TOK) for ref in (own_ref, below1_ref, below2_ref, below3_ref)]
    none = (jnp.ones((1, HK), F32), jnp.zeros((HV, HK), F32))

    def fold(way, below, order):
        found = none
        for k in order:
            passed = (place >= k) if below else (place < k)
            found = pick(passed, link(found, entries[k][way]), found)
        return found

    f_below, f_above = fold(0, True, (3, 2, 1)), fold(0, False, (3, 2, 1))
    b_above, b_below = fold(1, False, (1, 2, 3)), fold(1, True, (1, 2, 3))
    fwd = link(link(f_below, entries[0][0]), f_above)
    bwd = link(link(b_above, entries[0][1]), b_below)
    for n, pair in enumerate((fwd, bwd, f_below, b_above)):
        write_kept(kept_ref, n, pair)
    write_sent(sent_ref, fwd, bwd)


KEPT = jax.ShapeDtypeStruct((4, HV + 8, HK), F32)
SENT = jax.ShapeDtypeStruct((2 * HV + 16, HK), BF16)


def fold_x(place, packs):
    return pl.pallas_call(
        fold_body,
        in_specs=[SMEM] + [VMEM] * 4,
        out_specs=[VMEM, VMEM],
        out_shape=[KEPT, SENT],
        cost_estimate=cost(1 << 22),
        compiler_params=limit(4),
        name="fold_x",
    )(place, *packs)


def is_lower(place_ref, bit):
    return (place_ref[0] & bit) != 0


def met(lower, kept_ref, received_ref):
    fwd, bwd, before, after = (read_kept(kept_ref, n) for n in range(4))
    peer_f, peer_b = read_sent(received_ref, 0)
    return (
        pick(lower, link(peer_f, fwd), link(fwd, peer_f)),
        pick(lower, link(bwd, peer_b), link(peer_b, bwd)),
        pick(lower, link(peer_f, before), before),
        pick(lower, after, link(peer_b, after)),
    )


def merge_body(place_ref, kept_ref, received_ref, out_ref, sent_ref, *, bit):
    pairs = met(is_lower(place_ref, bit), kept_ref, received_ref)
    for n, pair in enumerate(pairs):
        write_kept(out_ref, n, pair)
    write_sent(sent_ref, pairs[0], pairs[1])


def merge(place, bit, kept, received):
    return pl.pallas_call(
        functools.partial(merge_body, bit=bit),
        in_specs=[SMEM, VMEM, VMEM],
        out_specs=[VMEM, VMEM],
        out_shape=[KEPT, SENT],
        cost_estimate=cost(1 << 22),
        compiler_params=limit(4),
        name="merge",
    )(place, kept, received)


def finish_body(
    place_ref, kept_ref, received_ref, out_ref, read_f_ref, read_b_ref, gain_ref, rows_ref, *, bit
):
    _, _, before, after = met(is_lower(place_ref, bit), kept_ref, received_ref)
    total = out_ref[...]
    for read_ref, (_, state) in ((read_f_ref, before), (read_b_ref, after)):
        total = total + lax.dot_general(
            read_ref[...], state.astype(BF16), (((1,), (1,)), ((), ())), preferred_element_type=F32
        )
    rows_ref[...] = rms_scale(total, gain_ref[...]).astype(BF16)


def finish(place, bit, kept, received, out, read_f, read_b, gain):
    return pl.pallas_call(
        functools.partial(finish_body, bit=bit),
        in_specs=[SMEM] + [VMEM] * 6,
        out_specs=VMEM,
        out_shape=jax.ShapeDtypeStruct((TOK, HV), BF16),
        cost_estimate=cost(1 << 25),
        compiler_params=limit(4),
        name="finish",
    )(place, kept, received, out, read_f, read_b, gain.reshape(1, HV))


def attend_tile(maps, kv_refs, peaks, accs, first):
    ones = jnp.ones((ACC_ROWS - AV, TOK), BF16)
    values = [
        jnp.concatenate(
            [
                jnp.concatenate(
                    [kv[TOK + n * 128 : TOK + (n + 1) * 128, :] for n in range(TOK // 128)], axis=1
                ),
                ones,
            ]
        )
        for kv in kv_refs
    ]
    accs, peaks, rises = list(accs), list(peaks), []
    units = [(m, n) for m in range(len(maps)) for n in range(len(kv_refs))]

    def scores_of(unit):
        return jnp.dot(kv_refs[unit[1]][:TOK, :], maps[unit[0]], preferred_element_type=F32)

    scores = scores_of(units[0])
    for at, (m, n) in enumerate(units):
        upcoming = scores_of(units[at + 1]) if at + 1 < len(units) else None
        if first:
            peaks[m] = jnp.max(scores, axis=0, keepdims=True)
        above = scores - peaks[m]
        if not first:
            rises.append(jnp.max(above.reshape(-1, 8, above.shape[1]), axis=0))
        added = jnp.dot(values[n], jnp.exp(above).astype(BF16), preferred_element_type=F32)
        accs[m] = added if first else accs[m] + added
        scores = upcoming
    return accs, peaks, None if first else jnp.max(functools.reduce(jnp.maximum, rises))


def attend_again(maps_ref, kv_refs, peaks_ref, accs_ref):
    ones = jnp.ones((ACC_ROWS - AV, 128), BF16)
    for kv in kv_refs:

        def absorb(i, unused):
            m, n = i // (TOK // 128), i % (TOK // 128)
            keys = kv[pl.ds(pl.multiple_of(n * 128, 128), 128), :]
            values = kv[pl.ds(pl.multiple_of(TOK + n * 128, 128), 128), :]
            scores = jnp.dot(keys, maps_ref[m], preferred_element_type=F32)
            old = peaks_ref[m, 0:1, :]
            new = jnp.maximum(old, jnp.max(scores, axis=0, keepdims=True))
            accs_ref[m] = accs_ref[m] * jnp.exp(old - new) + jnp.dot(
                jnp.concatenate([values, ones]),
                jnp.exp(scores - new).astype(BF16),
                preferred_element_type=F32,
            )
            peaks_ref[m, 0:1, :] = new
            return 0

        lax.fori_loop(0, 2 * TOK // 128, absorb, 0)


def both_maps(turned):
    upper = lax.broadcasted_iota(jnp.int32, turned.shape, 0) < AK
    zero = jnp.zeros_like(turned)
    return jnp.where(upper, turned, zero), jnp.where(upper, zero, turned)


def attend_first_body(*refs):
    q_refs, (kv_ref, turned_ref, peaks_ref, accs_ref) = refs[:NX], refs[NX:]
    for n, ref in enumerate(q_refs):
        turned_ref[n] = ref[:TOK, :].T

    def tile(t, unused):
        accs, peaks, _ = attend_tile(
            both_maps(turned_ref[t]), [kv_ref], [None] * 2, [None] * 2, True
        )
        for m in range(2):
            accs_ref[t, m] = accs[m]
            peaks_ref[t, m] = jnp.broadcast_to(peaks[m], (8, TOK))
        return 0

    lax.fori_loop(0, NX, tile, 0)


def attend_more_body(turned_ref, *refs, chunks):
    kv_refs, (peaks_in, accs_in, peaks_ref, accs_ref, maps_ref) = refs[:chunks], refs[chunks:]
    peaks_ref[...] = peaks_in[...]

    def tile(t, unused):
        maps = both_maps(turned_ref[t])
        peaks = [peaks_in[t, m, 0:1, :] for m in range(2)]
        accs, _, rise = attend_tile(maps, kv_refs, peaks, [accs_in[t, m] for m in range(2)], False)
        for m in range(2):
            accs_ref[t, m] = accs[m]

        @pl.when(rise > RISE)
        def _():
            maps_ref[0], maps_ref[1] = maps
            accs_ref[t] = accs_in[t]
            attend_again(maps_ref, kv_refs, peaks_ref.at[t], accs_ref.at[t])

        return 0

    lax.fori_loop(0, NX, tile, 0)


def attend_last_body(turned_ref, *refs, chunks, tile):
    kv_refs, rest = refs[:chunks], refs[chunks:]
    peaks_in, accs_in, *send_refs, peaks_ref, accs_ref, maps_ref, rise_ref = rest
    maps_ref[0], maps_ref[1] = both_maps(turned_ref[tile])
    peaks_ref[...] = peaks_in[tile]
    rise_ref[0] = 0.0

    def one_map(m, unused):
        accs, _, rise = attend_tile(
            [maps_ref[m]], kv_refs, [peaks_in[tile, m, 0:1, :]], [accs_in[tile, m]], False
        )
        accs_ref[m] = accs[0]
        rise_ref[0] = jnp.maximum(rise_ref[0], rise)
        return 0

    lax.fori_loop(0, 2, one_map, 0)

    @pl.when(rise_ref[0] > RISE)
    def _():
        accs_ref[...] = accs_in[tile]
        attend_again(maps_ref, kv_refs, peaks_ref, accs_ref)

    for m in range(2):
        acc = accs_ref[m]
        total = acc[AV : AV + 1, :]
        level = peaks_ref[m, 0:1, :] + jnp.log(total)
        high = level.astype(BF16)
        left = level - high.astype(F32)
        middle = left.astype(BF16)
        low = (left - middle.astype(F32)).astype(BF16)
        mean = (acc[:AV] * (1.0 / total)).astype(BF16)
        levels = jnp.concatenate(
            [high.astype(F32), middle.astype(F32), low.astype(F32), jnp.zeros((13, TOK), F32)]
        ).astype(BF16)
        ref = send_refs[m] if len(send_refs) > 1 else send_refs[0]
        at = 0 if len(send_refs) > 1 else m * MAP_ROWS
        ref[at : at + AV, :] = mean
        ref[at + AV : at + MAP_ROWS, :] = levels


STATE = [
    jax.ShapeDtypeStruct((NX, 2, 8, TOK), F32),
    jax.ShapeDtypeStruct((NX, 2, ACC_ROWS, TOK), F32),
]


def attend_cost(tiles, chunks):
    work = 2 * tiles * TOK * chunks * TOK
    return cost(work * 2 * (AK + AV), work)


def attend_first(packs, kv):
    return pl.pallas_call(
        attend_first_body,
        in_specs=[VMEM] * (NX + 1),
        out_specs=[VMEM] * 3,
        out_shape=[jax.ShapeDtypeStruct((NX, 2 * AK, TOK), BF16), *STATE],
        cost_estimate=attend_cost(NX, 1),
        compiler_params=limit(14),
        name="attend_first",
    )(*packs, kv)


def attend_more(turned, pieces, state):
    return pl.pallas_call(
        functools.partial(attend_more_body, chunks=len(pieces)),
        in_specs=[VMEM] * (len(pieces) + 3),
        out_specs=[VMEM] * 2,
        out_shape=STATE,
        scratch_shapes=[pltpu.VMEM((2, 2 * AK, TOK), BF16)],
        cost_estimate=attend_cost(NX, len(pieces)),
        compiler_params=limit(14),
        name="attend_more",
    )(turned, *pieces, *state)


def attend_last(turned, pieces, state, tile, parts):
    return pl.pallas_call(
        functools.partial(attend_last_body, chunks=len(pieces), tile=tile),
        in_specs=[VMEM] * (len(pieces) + 3),
        out_specs=[VMEM] * parts,
        out_shape=[jax.ShapeDtypeStruct((SEND_ROWS // parts, TOK), BF16)] * parts,
        scratch_shapes=[
            pltpu.VMEM((2, 8, TOK), F32),
            pltpu.VMEM((2, ACC_ROWS, TOK), F32),
            pltpu.VMEM((2, 2 * AK, TOK), BF16),
            pltpu.SMEM((1,), F32),
        ],
        cost_estimate=attend_cost(1, len(pieces)),
        compiler_params=limit(14),
        name="attend_last",
    )(turned, *pieces, *state)


SWAP = TOK // (NY * NC)


def mix_body(
    place_ref, rec_ref, a_ref, b_ref, c_ref, low_ref, high_ref, weight_ref, gain_ref,
    keep_ref, give_ref, att_ref,
):
    mixed = None
    for m in range(2):
        places = [(ref, m * MAP_ROWS) for ref in (a_ref, b_ref, c_ref)]
        places.append(((low_ref, high_ref)[m], 0))
        levels = []
        for ref, at in places:
            parts = ref[at + AV : at + MAP_ROWS, :].astype(F32)
            levels.append(parts[0:1] + parts[1:2] + parts[2:3])
        peak = functools.reduce(jnp.maximum, levels)
        shares = [jnp.exp(level - peak) for level in levels]
        scale = 1.0 / functools.reduce(jnp.add, shares)
        if m == 1:
            scale = scale * -weight_ref[0]
        for (ref, at), share in zip(places, shares):
            term = ref[at : at + AV, :].astype(F32) * (share * scale)
            mixed = term if mixed is None else mixed + term
    scale = lax.rsqrt(jnp.mean(mixed * mixed, axis=0, keepdims=True) + EPS)
    att_ref[...] = ((mixed * scale).T * gain_ref[...]).astype(BF16)
    y, c = place_ref[2], place_ref[3]
    for ref, core in ((keep_ref, c), (give_ref, 1 - c)):
        for k in range(NY):
            at = pl.multiple_of((((y + k) % NY) * NC + core) * SWAP, SWAP)
            ref[k, :, :HV] = rec_ref[pl.ds(at, SWAP), :]
            ref[k, :, HV:] = att_ref[pl.ds(at, SWAP), :]


def mix(place, rec_rows, partials, weight, gain):
    half = jax.ShapeDtypeStruct((NY, SWAP, HV + AV), BF16)
    return pl.pallas_call(
        mix_body,
        in_specs=[SMEM] + [VMEM] * 6 + [SMEM, VMEM],
        out_specs=[VMEM] * 2,
        out_shape=[half, half],
        scratch_shapes=[pltpu.VMEM((TOK, AV), BF16)],
        cost_estimate=cost(1 << 22),
        compiler_params=limit(6),
        name="mix",
    )(place, rec_rows, *partials, weight, gain.reshape(1, AV))


def join_body(place_ref, keep_ref, got_ref, *out_refs):
    first = place_ref[3] == 0
    for k, ref in enumerate(out_refs):
        keep, got = keep_ref[k], got_ref[k]
        low, high = jnp.where(first, keep, got), jnp.where(first, got, keep)
        ref[:, :HV], ref[:, HV : 2 * HV] = low[:, :HV], high[:, :HV]
        ref[:, 2 * HV : 2 * HV + AV], ref[:, 2 * HV + AV :] = low[:, HV:], high[:, HV:]


def join(place, keep, got):
    return pl.pallas_call(
        join_body,
        in_specs=[SMEM, VMEM, VMEM],
        out_specs=[VMEM] * NY,
        out_shape=[jax.ShapeDtypeStruct((SWAP, 2 * (HV + AV)), BF16)] * NY,
        cost_estimate=cost(1 << 20),
        compiler_params=limit(2),
        name="join",
    )(place, keep, got)


def project_body(place_ref, *refs):
    sources, (rec_ref, att_ref, out_ref) = refs[:NY], refs[NY:]
    total = None
    for weights_ref, width, start in ((rec_ref, 2 * HV, 0), (att_ref, 2 * AV, 2 * HV)):
        for k, ref in enumerate(sources):
            at = pl.multiple_of(((place_ref[2] + NY - k) % NY) * width, width)
            term = jnp.dot(
                ref[:, start : start + width],
                weights_ref[pl.ds(at, width), :],
                preferred_element_type=F32,
            )
            total = term if total is None else total + term
    out_ref[...] = total.astype(BF16)


def project(place, sources, out_rec, out_att):
    return pl.pallas_call(
        project_body,
        in_specs=[SMEM] + [VMEM] * (NY + 2),
        out_specs=VMEM,
        out_shape=jax.ShapeDtypeStruct((SWAP, out_rec.shape[1]), BF16),
        cost_estimate=cost(1 << 29),
        compiler_params=limit(6),
        name="project",
    )(place, *sources, out_rec, out_att)


def on_device(
    tokens,
    norm_gain,
    rec_query,
    fwd_gate,
    bwd_gate,
    rec_value,
    gate_leak,
    log_decay,
    rec_gain,
    att_query,
    att_key,
    att_value,
    lambdas,
    att_gain,
    out_rec,
    out_att,
):
    place = jnp.stack([lax.axis_index(axis) for axis in AXES]).astype(jnp.int32)
    decays = jnp.broadcast_to(log_decay, (2, TOK, 128))
    cosine, sine = rotation_tables(TOK)
    normed = rms_scale(tokens.astype(F32), norm_gain).astype(BF16)
    mine, other = gather_rows(normed)
    rows, own_kv = make_keys(place, mine, other, att_key, att_value, cosine, sine)
    ups, downs = [own_kv], [own_kv]
    for step in range(1, NZ // 2 + 1):
        ups.append(shift(ups[-1], "z", 1, NZ))
        if step < NZ // 2:
            downs.append(shift(downs[-1], "z", -1, NZ))
    pack, out_local, read_f, read_b = make_local(
        rows,
        (att_query, rec_query, fwd_gate, bwd_gate, rec_value),
        gate_leak,
        decays,
        cosine,
        sine,
    )
    packs = [pack]
    for by in (1, 2, -1):
        packs.append(shift(pack, "x", by, NX))
    kept, sent = fold_x(place, packs)
    turned, *state = attend_first([packs[0], packs[1], packs[3], packs[2]], own_kv)
    for bit in (1, 2, 4):
        received = lax.ppermute(sent, "z", [(i, i ^ bit) for i in range(NZ)])
        if bit < 4:
            kept, sent = merge(place, bit, kept, received)
    state = attend_more(turned, [ups[1], downs[1]], state)
    state = attend_more(turned, [ups[2], downs[2]], state)
    ends = [ups[3], downs[3], ups[4]]
    low, high = attend_last(turned, ends, state, 3, 2)
    far_low = shift(low, "x", 2, NX)
    far_high = shift(high, "x", -2, NX)
    (send,) = attend_last(turned, ends, state, 1, 1)
    from_above = shift(send, "x", -1, NX)
    (send,) = attend_last(turned, ends, state, 2, 1)
    from_below = shift(send, "x", 1, NX)
    (own,) = attend_last(turned, ends, state, 0, 1)
    rec_rows = finish(place, bit, kept, received, out_local, read_f, read_b, rec_gain)
    partials = [own, from_above, from_below, far_low, far_high]
    keep, give = mix(place, rec_rows, partials, lambdas, att_gain)
    got = shift(give, "c", 1, NC)
    joined = join(place, keep, got)
    sources = [joined[0]]
    for k in range(1, NY):
        sources.append(shift(joined[k], "y", k, NY))
    return project(place, sources, out_rec, out_att)


def solution(mesh):
    torus = Mesh(mesh.devices.reshape(NZ, NX, NY, NC), AXES)
    in_specs = (
        P(AXES, None),
        P(),
        P(None, TP),
        P(None, TP),
        P(None, TP),
        P(None, TP),
        P(None, TP),
        P(None, SP, TP),
        P(),
        P(None, TP),
        P(None, TP),
        P(None, TP),
        P(TP),
        P(),
        P(),
        P(),
    )
    out_specs = P(AXES, None)
    return jax.shard_map(
        on_device, mesh=torus, in_specs=in_specs, out_specs=out_specs, check_vma=False
    )
```

```python
import functools

import jax
import jax.numpy as jnp
from jax import lax
from jax.experimental import pallas as pl
from jax.experimental.pallas import tpu as pltpu
from jax.sharding import Mesh
from jax.sharding import PartitionSpec as P


HK = 128
HV = 128
AK = 64
AV = 128
BLOCK = 64
NZ, NX, NY, NC = 8, 4, 4, 2
AXES = ("z", "x", "y", "c")
SP = ("z", "x")
TP = ("y", "c")
TOK = 512
ACC_ROWS = 144
MAP_ROWS = AV + 16
SEND_ROWS = 2 * MAP_ROWS
PACK = 784
BF16 = jnp.bfloat16
F32 = jnp.float32

EPS = 1e-06
THETA = 500000.0
RISE = 40.0
LOW = -1e30
PEERS = NX - 1
FAR = 384


def shift(value, axis, by, size):
    return lax.ppermute(value, axis, [(i, (i + by) % size) for i in range(size)])


def gather_rows(rows):
    half = rows.shape[0] // 2
    far_low = shift(rows[:half], "y", 2, NY)
    far_high = shift(rows[half:], "y", -2, NY)
    up = shift(rows, "y", 1, NY)
    down = shift(rows, "y", -1, NY)
    mine = jnp.concatenate([rows, up, down, far_low, far_high])
    return mine, shift(mine, "c", 1, NC)


def rms_scale(values, gain):
    return values * lax.rsqrt(jnp.mean(values * values, axis=-1, keepdims=True) + EPS) * gain


VMEM = pl.BlockSpec(memory_space=pltpu.VMEM)
SMEM = pl.BlockSpec(memory_space=pltpu.SMEM)


def limit(mib):
    return pltpu.CompilerParams(vmem_limit_bytes=mib << 20)


def cost(flops, transcendentals=0):
    return pl.CostEstimate(flops=flops, transcendentals=transcendentals, bytes_accessed=1 << 20)


def rotation_tables(length):
    positions = (lax.axis_index(SP) * length + jnp.arange(length, dtype=jnp.int32)).astype(F32)
    frequency = THETA ** (-(jnp.arange(AK // 2, dtype=F32) * 2.0 / AK))
    angles = positions[:, None] * frequency[None, :]
    cosine, sine = jnp.cos(angles), jnp.sin(angles)
    return (
        jnp.concatenate([cosine] * 4, axis=1),
        jnp.concatenate([-sine, sine, -sine, sine], axis=1),
    )


def rotated(vectors, cosine, sine):
    lane = lax.broadcasted_iota(jnp.int32, vectors.shape, 1)
    half = AK // 2
    partner = jnp.where(
        (lane & half) == 0, pltpu.roll(vectors, 128 - half, 1), pltpu.roll(vectors, half, 1)
    )
    return vectors * cosine + partner * sine


def keys_body(
    place_ref, mine_ref, other_ref, key_ref, value_ref, cos_ref, sin_ref, rows_ref, out_ref
):
    y, c = place_ref[2], place_ref[3]
    size = mine_ref.shape[0] // NY
    for core, ref in ((c, mine_ref), (1 - c, other_ref)):
        for n, distance in enumerate((0, 3, 1, 2)):
            at = pl.multiple_of((((y + distance) % NY) * NC + core) * size, size)
            rows_ref[pl.ds(at, size), :] = ref[n * size : (n + 1) * size, :]
    weights = jnp.concatenate([key_ref[...], value_ref[...]], axis=1)
    raw = jnp.dot(rows_ref[...], weights, preferred_element_type=F32).astype(BF16)
    out_ref[:TOK, :] = rotated(raw[:, :128].astype(F32), cos_ref[...], sin_ref[...]).astype(BF16)
    for n in range(TOK // 128):
        out_ref[TOK + n * 128 : TOK + (n + 1) * 128, :] = raw[n * 128 : (n + 1) * 128, 128:].T


def make_keys(place, mine, other, key, value, cosine, sine):
    return pl.pallas_call(
        keys_body,
        in_specs=[SMEM] + [VMEM] * 6,
        out_specs=[VMEM, VMEM],
        out_shape=[
            jax.ShapeDtypeStruct((TOK, mine.shape[1]), BF16),
            jax.ShapeDtypeStruct((2 * TOK, 128), BF16),
        ],
        cost_estimate=cost(1 << 29),
        compiler_params=limit(6),
        name="make_keys",
    )(place, mine, other, key, value, cosine, sine)


def local_body(
    rows_ref, aq_ref, q_ref, f_ref, b_ref, v_ref, leak_ref, decay_ref, cos_ref, sin_ref,
    pack_ref, far_a_ref, far_b_ref, out_ref, read_f_ref, read_b_ref,
):
    def project(*weights):
        joined = jnp.concatenate([w[...] for w in weights], axis=1)
        return jnp.dot(rows_ref[...], joined, preferred_element_type=F32).astype(BF16)

    raw_f_b = project(f_ref, b_ref)
    raw_q_v = project(q_ref, v_ref)
    raw_aq = project(aq_ref)
    pack_ref[:TOK, :] = (
        rotated(raw_aq.astype(F32), cos_ref[...], sin_ref[...]) * AK ** (-0.5)
    ).astype(BF16)
    raw = raw_q_v[:, :128].astype(F32)
    queries = raw / (1.0 + jnp.exp(-raw))
    row = lax.broadcasted_iota(jnp.int32, (BLOCK, BLOCK), 0)
    col = lax.broadcasted_iota(jnp.int32, (BLOCK, BLOCK), 1)
    totals = []
    for way, read_ref in enumerate((read_f_ref, read_b_ref)):
        gates = raw_f_b[:, way * HK : (way + 1) * HK].astype(F32)
        keys = leak_ref[way : way + 1, :] / (1.0 + jnp.exp(gates))
        logs = jnp.log1p(-keys) + decay_ref[way]
        reach = (row >= col) if way == 0 else (row <= col)
        sums = jnp.where(reach, 1.0, 0.0)
        middle_row, last_row = (BLOCK // 2 - 1, BLOCK - 1) if way == 0 else (BLOCK // 2, 0)
        state = jnp.zeros((HV, HK), F32)
        before = jnp.zeros((1, HK), F32)
        blocks = range(TOK // BLOCK)
        for n in blocks if way == 0 else reversed(blocks):
            at = slice(n * BLOCK, (n + 1) * BLOCK)
            cumulative = jnp.dot(
                sums, logs[at], precision=lax.Precision.HIGHEST, preferred_element_type=F32
            )
            middle = cumulative[middle_row : middle_row + 1]
            last = cumulative[last_row : last_row + 1]
            scores = lax.dot_general(
                (queries[at] * jnp.exp(cumulative - middle)).astype(BF16),
                (keys[at] * jnp.exp(middle - cumulative)).astype(BF16),
                (((1,), (1,)), ((), ())),
                preferred_element_type=F32,
            )
            scores = jnp.where(reach, scores, 0.0).astype(BF16)
            values = raw_q_v[at, 128:]
            out = jnp.dot(scores, values, preferred_element_type=F32)
            read = queries[at] * jnp.exp(cumulative)
            out = out + lax.dot_general(
                read.astype(BF16),
                state.astype(BF16),
                (((1,), (1,)), ((), ())),
                preferred_element_type=F32,
            )
            out_ref[at, :] = out if way == 0 else out_ref[at, :] + out
            read_ref[at, :] = (read * jnp.exp(before)).astype(BF16)
            added = lax.dot_general(
                values,
                (keys[at] * jnp.exp(last - cumulative)).astype(BF16),
                (((0,), (0,)), ((), ())),
                preferred_element_type=F32,
            )
            state = state * jnp.exp(last) + added
            before = before + last
        pack_ref[TOK + way * HV : TOK + (way + 1) * HV, :] = state.astype(BF16)
        totals.append(jnp.exp(before))
    pack_ref[TOK + 2 * HV :, :] = jnp.concatenate(
        [*totals, jnp.zeros((PACK - TOK - 2 * HV - 2, HK), F32)]
    ).astype(BF16)
    far_a_ref[...] = pack_ref[:FAR, :]
    far_b_ref[...] = pack_ref[FAR:, :]


def make_local(rows, weights, leak, decays, cosine, sine):
    return pl.pallas_call(
        local_body,
        in_specs=[VMEM] * 10,
        out_specs=[VMEM] * 6,
        out_shape=[
            jax.ShapeDtypeStruct((PACK, 128), BF16),
            jax.ShapeDtypeStruct((FAR, 128), BF16),
            jax.ShapeDtypeStruct((PACK - FAR, 128), BF16),
            jax.ShapeDtypeStruct((TOK, 128), F32),
            jax.ShapeDtypeStruct((TOK, 128), BF16),
            jax.ShapeDtypeStruct((TOK, 128), BF16),
        ],
        cost_estimate=cost(1 << 31),
        compiler_params=limit(12),
        name="local",
    )(rows, *weights, leak, decays, cosine, sine)


def link(earlier, later):
    return (earlier[0] * later[0], later[0] * earlier[1] + later[1])


def pick(condition, new, old):
    return tuple(jnp.where(condition, a, b) for a, b in zip(new, old))


def read_sent(ref, at):
    decays = ref[at + 2 * HV : at + 2 * HV + 16, :].astype(F32)
    return (
        (decays[0:1], ref[at : at + HV, :].astype(F32)),
        (decays[1:2], ref[at + HV : at + 2 * HV, :].astype(F32)),
    )


def write_sent(ref, fwd, bwd):
    ref[:HV, :] = fwd[1].astype(BF16)
    ref[HV : 2 * HV, :] = bwd[1].astype(BF16)
    ref[2 * HV :, :] = jnp.concatenate([fwd[0], bwd[0], jnp.zeros((14, HK), F32)]).astype(BF16)


def write_kept(ref, n, pair):
    ref[n, :HV, :] = pair[1]
    ref[n, HV:, :] = jnp.broadcast_to(pair[0], (8, HK))


def read_kept(ref, n):
    return ref[n, HV : HV + 1, :], ref[n, :HV, :]


def fold_body(place_ref, own_ref, below1_ref, below2_ref, below3_ref, kept_ref, sent_ref):
    place = place_ref[1]
    entries = [
        read_sent(own_ref, TOK),
        read_sent(below1_ref, TOK),
        read_sent(below2_ref, TOK - FAR),
        read_sent(below3_ref, TOK),
    ]
    none = (jnp.ones((1, HK), F32), jnp.zeros((HV, HK), F32))

    def fold(way, below, order):
        found = none
        for k in order:
            passed = (place >= k) if below else (place < k)
            found = pick(passed, link(found, entries[k][way]), found)
        return found

    f_below, f_above = fold(0, True, (3, 2, 1)), fold(0, False, (3, 2, 1))
    b_above, b_below = fold(1, False, (1, 2, 3)), fold(1, True, (1, 2, 3))
    fwd = link(link(f_below, entries[0][0]), f_above)
    bwd = link(link(b_above, entries[0][1]), b_below)
    for n, pair in enumerate((fwd, bwd, f_below, b_above)):
        write_kept(kept_ref, n, pair)
    write_sent(sent_ref, fwd, bwd)


KEPT = jax.ShapeDtypeStruct((4, HV + 8, HK), F32)
SENT = jax.ShapeDtypeStruct((2 * HV + 16, HK), BF16)


def fold_x(place, packs):
    return pl.pallas_call(
        fold_body,
        in_specs=[SMEM] + [VMEM] * 4,
        out_specs=[VMEM, VMEM],
        out_shape=[KEPT, SENT],
        cost_estimate=cost(1 << 22),
        compiler_params=limit(4),
        name="fold_x",
    )(place, *packs)


def is_lower(place_ref, bit):
    return (place_ref[0] & bit) != 0


def met(lower, kept_ref, received_ref):
    fwd, bwd, before, after = (read_kept(kept_ref, n) for n in range(4))
    peer_f, peer_b = read_sent(received_ref, 0)
    return (
        pick(lower, link(peer_f, fwd), link(fwd, peer_f)),
        pick(lower, link(bwd, peer_b), link(peer_b, bwd)),
        pick(lower, link(peer_f, before), before),
        pick(lower, after, link(peer_b, after)),
    )


def merge_body(place_ref, kept_ref, received_ref, out_ref, sent_ref, *, bit):
    pairs = met(is_lower(place_ref, bit), kept_ref, received_ref)
    for n, pair in enumerate(pairs):
        write_kept(out_ref, n, pair)
    write_sent(sent_ref, pairs[0], pairs[1])


def merge(place, bit, kept, received):
    return pl.pallas_call(
        functools.partial(merge_body, bit=bit),
        in_specs=[SMEM, VMEM, VMEM],
        out_specs=[VMEM, VMEM],
        out_shape=[KEPT, SENT],
        cost_estimate=cost(1 << 22),
        compiler_params=limit(4),
        name="merge",
    )(place, kept, received)


def finish_body(
    place_ref, kept_ref, received_ref, out_ref, read_f_ref, read_b_ref, gain_ref, rows_ref, *, bit
):
    _, _, before, after = met(is_lower(place_ref, bit), kept_ref, received_ref)
    total = out_ref[...]
    for read_ref, (_, state) in ((read_f_ref, before), (read_b_ref, after)):
        total = total + lax.dot_general(
            read_ref[...], state.astype(BF16), (((1,), (1,)), ((), ())), preferred_element_type=F32
        )
    rows_ref[...] = rms_scale(total, gain_ref[...]).astype(BF16)


def finish(place, bit, kept, received, out, read_f, read_b, gain):
    return pl.pallas_call(
        functools.partial(finish_body, bit=bit),
        in_specs=[SMEM] + [VMEM] * 6,
        out_specs=VMEM,
        out_shape=jax.ShapeDtypeStruct((TOK, HV), BF16),
        cost_estimate=cost(1 << 25),
        compiler_params=limit(4),
        name="finish",
    )(place, kept, received, out, read_f, read_b, gain.reshape(1, HV))


def attend_tile(maps, kv_refs, peaks, accs):
    ones = jnp.ones((ACC_ROWS - AV, TOK), BF16)
    values = [
        jnp.concatenate(
            [
                jnp.concatenate(
                    [kv[TOK + n * 128 : TOK + (n + 1) * 128, :] for n in range(TOK // 128)], axis=1
                ),
                ones,
            ]
        )
        for kv in kv_refs
    ]
    accs, peaks, rises = list(accs), list(peaks), []
    units = [(m, n) for m in range(len(maps)) for n in range(len(kv_refs))]

    def scores_of(unit):
        return jnp.dot(kv_refs[unit[1]][:TOK, :], maps[unit[0]], preferred_element_type=F32)

    scores = scores_of(units[0])
    for at, (m, n) in enumerate(units):
        upcoming = scores_of(units[at + 1]) if at + 1 < len(units) else None
        found = peaks[m] is None
        if found:
            peaks[m] = jnp.max(scores, axis=0, keepdims=True)
        above = scores - peaks[m]
        if not found:
            rises.append(jnp.max(above.reshape(-1, 8, above.shape[1]), axis=0))
        added = jnp.dot(values[n], jnp.exp(above).astype(BF16), preferred_element_type=F32)
        accs[m] = added if accs[m] is None else accs[m] + added
        scores = upcoming
    return accs, peaks, jnp.max(functools.reduce(jnp.maximum, rises)) if rises else None


def attend_again(maps_ref, kv_refs, peaks_ref, accs_ref):
    ones = jnp.ones((ACC_ROWS - AV, 128), BF16)
    steps = TOK // 128
    for kv in kv_refs:

        def absorb(i, unused):
            m, w, n = i // (steps * steps), (i // steps) % steps, i % steps
            keys = kv[pl.ds(pl.multiple_of(n * 128, 128), 128), :]
            values = kv[pl.ds(pl.multiple_of(TOK + n * 128, 128), 128), :]
            cols = pl.ds(pl.multiple_of(w * 128, 128), 128)
            scores = jnp.dot(keys, maps_ref[m, :, cols], preferred_element_type=F32)
            old = peaks_ref[m, 0:1, cols]
            new = jnp.maximum(old, jnp.max(scores, axis=0, keepdims=True))
            accs_ref[m, :, cols] = accs_ref[m, :, cols] * jnp.exp(old - new) + jnp.dot(
                jnp.concatenate([values, ones]),
                jnp.exp(scores - new).astype(BF16),
                preferred_element_type=F32,
            )
            peaks_ref[m, 0:1, cols] = new
            return 0

        lax.fori_loop(0, 2 * steps * steps, absorb, 0)


def both_maps(turned):
    upper = lax.broadcasted_iota(jnp.int32, turned.shape, 0) < AK
    zero = jnp.zeros_like(turned)
    return jnp.where(upper, turned, zero), jnp.where(upper, zero, turned)


def attend_first_body(below_ref, above_ref, far_a_ref, far_b_ref, kv_ref, turned_ref, peaks_ref, accs_ref):
    turned_ref[0] = below_ref[:TOK, :].T
    turned_ref[1] = above_ref[:TOK, :].T
    turned_ref[2] = jnp.concatenate([far_a_ref[...], far_b_ref[: TOK - FAR, :]]).T

    def tile(t, unused):
        accs, peaks, _ = attend_tile(both_maps(turned_ref[t]), [kv_ref], [None] * 2, [None] * 2)
        for m in range(2):
            accs_ref[t, m] = accs[m]
            peaks_ref[t, m] = jnp.broadcast_to(peaks[m], (8, TOK))
        return 0

    lax.fori_loop(0, PEERS, tile, 0)


def attend_more_body(turned_ref, *refs, chunks):
    kv_refs, (peaks_in, accs_in, peaks_ref, accs_ref, maps_ref) = refs[:chunks], refs[chunks:]
    peaks_ref[...] = peaks_in[...]

    def tile(t, unused):
        maps = both_maps(turned_ref[t])
        peaks = [peaks_in[t, m, 0:1, :] for m in range(2)]
        accs, _, rise = attend_tile(maps, kv_refs, peaks, [accs_in[t, m] for m in range(2)])
        for m in range(2):
            accs_ref[t, m] = accs[m]

        @pl.when(rise > RISE)
        def _():
            maps_ref[0], maps_ref[1] = maps
            accs_ref[t] = accs_in[t]
            attend_again(maps_ref, kv_refs, peaks_ref.at[t], accs_ref.at[t])

        return 0

    lax.fori_loop(0, PEERS, tile, 0)


def write_partial(send_refs, peaks_ref, accs_ref):
    for m in range(2):
        acc = accs_ref[m]
        total = acc[AV : AV + 1, :]
        level = peaks_ref[m, 0:1, :] + jnp.log(total)
        high = level.astype(BF16)
        left = level - high.astype(F32)
        middle = left.astype(BF16)
        low = (left - middle.astype(F32)).astype(BF16)
        mean = (acc[:AV] * (1.0 / total)).astype(BF16)
        levels = jnp.concatenate(
            [high.astype(F32), middle.astype(F32), low.astype(F32), jnp.zeros((13, TOK), F32)]
        ).astype(BF16)
        ref = send_refs[m] if len(send_refs) > 1 else send_refs[0]
        at = 0 if len(send_refs) > 1 else m * MAP_ROWS
        ref[at : at + AV, :] = mean
        ref[at + AV : at + MAP_ROWS, :] = levels


def attend_last_body(turned_ref, *refs, chunks, tiles):
    kv_refs, rest = refs[:chunks], refs[chunks:]
    peaks_in, accs_in, *send_refs, peaks_ref, accs_ref, maps_ref, rise_ref = rest
    start, count = tiles
    for t in range(count):
        maps_ref[t, 0], maps_ref[t, 1] = both_maps(turned_ref[start + t])
        rise_ref[t] = 0.0

    def one_map(i, unused):
        t, m = i // 2, i % 2
        peaks = peaks_in[start + t, m]
        accs, _, rise = attend_tile(
            [maps_ref[t, m]], kv_refs, [peaks[0:1]], [accs_in[start + t, m]]
        )
        peaks_ref[t, m] = peaks
        accs_ref[t, m] = accs[0]
        rise_ref[t] = jnp.maximum(rise_ref[t], rise)
        return 0

    lax.fori_loop(0, 2 * count, one_map, 0)

    def check(t, unused):
        @pl.when(rise_ref[t] > RISE)
        def _():
            accs_ref[t] = accs_in[start + t]
            attend_again(maps_ref.at[t], kv_refs, peaks_ref.at[t], accs_ref.at[t])

        return 0

    lax.fori_loop(0, count, check, 0)
    parts = len(send_refs) // count
    for t in range(count):
        write_partial(send_refs[t * parts : (t + 1) * parts], peaks_ref.at[t], accs_ref.at[t])


def attend_own_body(pack_ref, *refs, chunks):
    kv_refs, (own_ref, peaks_ref, accs_ref, maps_ref, rise_ref) = refs[:chunks], refs[chunks:]
    maps_ref[0, 0], maps_ref[0, 1] = both_maps(pack_ref[:TOK, :].T)
    rise_ref[0] = 0.0

    def one_map(m, unused):
        accs, peaks, rise = attend_tile([maps_ref[0, m]], kv_refs, [None], [None])
        accs_ref[0, m] = accs[0]
        peaks_ref[0, m] = jnp.broadcast_to(peaks[0], (8, TOK))
        rise_ref[0] = jnp.maximum(rise_ref[0], rise)
        return 0

    lax.fori_loop(0, 2, one_map, 0)

    @pl.when(rise_ref[0] > RISE)
    def _():
        peaks_ref[...] = jnp.full(peaks_ref.shape, LOW, F32)
        accs_ref[...] = jnp.zeros(accs_ref.shape, F32)
        attend_again(maps_ref.at[0], kv_refs, peaks_ref.at[0], accs_ref.at[0])

    write_partial([own_ref], peaks_ref.at[0], accs_ref.at[0])


STATE = [
    jax.ShapeDtypeStruct((PEERS, 2, 8, TOK), F32),
    jax.ShapeDtypeStruct((PEERS, 2, ACC_ROWS, TOK), F32),
]


def tile_scratch(count):
    return [
        pltpu.VMEM((count, 2, 8, TOK), F32),
        pltpu.VMEM((count, 2, ACC_ROWS, TOK), F32),
        pltpu.VMEM((count, 2, 2 * AK, TOK), BF16),
        pltpu.SMEM((count,), F32),
    ]


def attend_cost(tiles, chunks):
    work = 2 * tiles * TOK * chunks * TOK
    return cost(work * 2 * (AK + AV), work)


def attend_first(*operands):
    return pl.pallas_call(
        attend_first_body,
        in_specs=[VMEM] * 5,
        out_specs=[VMEM] * 3,
        out_shape=[jax.ShapeDtypeStruct((PEERS, 2 * AK, TOK), BF16), *STATE],
        cost_estimate=attend_cost(PEERS, 1),
        compiler_params=limit(14),
        name="attend_first",
    )(*operands)


def attend_more(turned, pieces, state):
    return pl.pallas_call(
        functools.partial(attend_more_body, chunks=len(pieces)),
        in_specs=[VMEM] * (len(pieces) + 3),
        out_specs=[VMEM] * 2,
        out_shape=STATE,
        scratch_shapes=[pltpu.VMEM((2, 2 * AK, TOK), BF16)],
        cost_estimate=attend_cost(PEERS, len(pieces)),
        compiler_params=limit(14),
        name="attend_more",
    )(turned, *pieces, *state)


def attend_last(turned, pieces, state, tiles, parts):
    count = tiles[1]
    return pl.pallas_call(
        functools.partial(attend_last_body, chunks=len(pieces), tiles=tiles),
        in_specs=[VMEM] * (len(pieces) + 3),
        out_specs=[VMEM] * (parts * count),
        out_shape=[jax.ShapeDtypeStruct((SEND_ROWS // parts, TOK), BF16)] * (parts * count),
        scratch_shapes=tile_scratch(count),
        cost_estimate=attend_cost(count, len(pieces)),
        compiler_params=limit(14),
        name="attend_last",
    )(turned, *pieces, *state)


def attend_own(pack, pieces):
    return pl.pallas_call(
        functools.partial(attend_own_body, chunks=len(pieces)),
        in_specs=[VMEM] * (len(pieces) + 1),
        out_specs=VMEM,
        out_shape=jax.ShapeDtypeStruct((SEND_ROWS, TOK), BF16),
        scratch_shapes=tile_scratch(1),
        cost_estimate=attend_cost(1, len(pieces)),
        compiler_params=limit(14),
        name="attend_own",
    )(pack, *pieces)


SWAP = TOK // (NY * NC)


def mix_body(
    place_ref, rec_ref, a_ref, b_ref, c_ref, low_ref, high_ref, weight_ref, gain_ref,
    keep_ref, give_ref, att_ref,
):
    mixed = None
    for m in range(2):
        places = [(ref, m * MAP_ROWS) for ref in (a_ref, b_ref, c_ref)]
        places.append(((low_ref, high_ref)[m], 0))
        levels = []
        for ref, at in places:
            parts = ref[at + AV : at + MAP_ROWS, :].astype(F32)
            levels.append(parts[0:1] + parts[1:2] + parts[2:3])
        peak = functools.reduce(jnp.maximum, levels)
        shares = [jnp.exp(level - peak) for level in levels]
        scale = 1.0 / functools.reduce(jnp.add, shares)
        if m == 1:
            scale = scale * -weight_ref[0]
        for (ref, at), share in zip(places, shares):
            term = ref[at : at + AV, :].astype(F32) * (share * scale)
            mixed = term if mixed is None else mixed + term
    scale = lax.rsqrt(jnp.mean(mixed * mixed, axis=0, keepdims=True) + EPS)
    att_ref[...] = ((mixed * scale).T * gain_ref[...]).astype(BF16)
    y, c = place_ref[2], place_ref[3]
    for ref, core in ((keep_ref, c), (give_ref, 1 - c)):
        for k in range(NY):
            at = pl.multiple_of((((y + k) % NY) * NC + core) * SWAP, SWAP)
            ref[k, :, :HV] = rec_ref[pl.ds(at, SWAP), :]
            ref[k, :, HV:] = att_ref[pl.ds(at, SWAP), :]


def mix(place, rec_rows, partials, weight, gain):
    half = jax.ShapeDtypeStruct((NY, SWAP, HV + AV), BF16)
    return pl.pallas_call(
        mix_body,
        in_specs=[SMEM] + [VMEM] * 6 + [SMEM, VMEM],
        out_specs=[VMEM] * 2,
        out_shape=[half, half],
        scratch_shapes=[pltpu.VMEM((TOK, AV), BF16)],
        cost_estimate=cost(1 << 22),
        compiler_params=limit(6),
        name="mix",
    )(place, rec_rows, *partials, weight, gain.reshape(1, AV))


def join_body(place_ref, keep_ref, got_ref, *out_refs):
    first = place_ref[3] == 0
    for k, ref in enumerate(out_refs):
        keep, got = keep_ref[k], got_ref[k]
        low, high = jnp.where(first, keep, got), jnp.where(first, got, keep)
        ref[:, :HV], ref[:, HV : 2 * HV] = low[:, :HV], high[:, :HV]
        ref[:, 2 * HV : 2 * HV + AV], ref[:, 2 * HV + AV :] = low[:, HV:], high[:, HV:]


def join(place, keep, got):
    return pl.pallas_call(
        join_body,
        in_specs=[SMEM, VMEM, VMEM],
        out_specs=[VMEM] * NY,
        out_shape=[jax.ShapeDtypeStruct((SWAP, 2 * (HV + AV)), BF16)] * NY,
        cost_estimate=cost(1 << 20),
        compiler_params=limit(2),
        name="join",
    )(place, keep, got)


def project_body(place_ref, *refs):
    sources, (rec_ref, att_ref, out_ref, rows_ref) = refs[:NY], refs[NY:]
    for k, ref in enumerate(sources):
        at = pl.multiple_of(((place_ref[2] + NY - k) % NY) * 2 * HV, 2 * HV)
        for n in range(2):
            rows_ref[n, :, pl.ds(at, 2 * HV)] = ref[:, n * 2 * HV : (n + 1) * 2 * HV]
    total = jnp.dot(rows_ref[0], rec_ref[...], preferred_element_type=F32)
    total = total + jnp.dot(rows_ref[1], att_ref[...], preferred_element_type=F32)
    out_ref[...] = total.astype(BF16)


def project(place, sources, out_rec, out_att):
    return pl.pallas_call(
        project_body,
        in_specs=[SMEM] + [VMEM] * (NY + 2),
        out_specs=VMEM,
        out_shape=jax.ShapeDtypeStruct((SWAP, out_rec.shape[1]), BF16),
        scratch_shapes=[pltpu.VMEM((2, SWAP, 2 * NY * HV), BF16)],
        cost_estimate=cost(1 << 29),
        compiler_params=limit(6),
        name="project",
    )(place, *sources, out_rec, out_att)


def on_device(
    tokens,
    norm_gain,
    rec_query,
    fwd_gate,
    bwd_gate,
    rec_value,
    gate_leak,
    log_decay,
    rec_gain,
    att_query,
    att_key,
    att_value,
    lambdas,
    att_gain,
    out_rec,
    out_att,
):
    place = jnp.stack([lax.axis_index(axis) for axis in AXES]).astype(jnp.int32)
    decays = jnp.broadcast_to(log_decay, (2, TOK, 128))
    cosine, sine = rotation_tables(TOK)
    normed = rms_scale(tokens.astype(F32), norm_gain).astype(BF16)
    mine, other = gather_rows(normed)
    rows, own_kv = make_keys(place, mine, other, att_key, att_value, cosine, sine)
    ups, downs = [own_kv], [own_kv]
    for step in range(1, NZ // 2 + 1):
        ups.append(shift(ups[-1], "z", 1, NZ))
        if step < NZ // 2:
            downs.append(shift(downs[-1], "z", -1, NZ))
    pack, far_a, far_b, out_local, read_f, read_b = make_local(
        rows,
        (att_query, rec_query, fwd_gate, bwd_gate, rec_value),
        gate_leak,
        decays,
        cosine,
        sine,
    )
    far_a = shift(far_a, "x", 2, NX)
    far_b = shift(far_b, "x", -2, NX)
    below = shift(pack, "x", 1, NX)
    above = shift(pack, "x", -1, NX)
    kept, sent = fold_x(place, [pack, below, far_b, above])
    turned, *state = attend_first(below, above, far_a, far_b, own_kv)
    for bit in (1, 2, 4):
        received = lax.ppermute(sent, "z", [(i, i ^ bit) for i in range(NZ)])
        if bit < 4:
            kept, sent = merge(place, bit, kept, received)
    state = attend_more(turned, [ups[1], downs[1]], state)
    state = attend_more(turned, [ups[2], downs[2]], state)
    ends = [ups[3], downs[3], ups[4]]
    low, high = attend_last(turned, ends, state, (2, 1), 2)
    far_low = shift(low, "x", 2, NX)
    far_high = shift(high, "x", -2, NX)
    to_below, to_above = attend_last(turned, ends, state, (0, 2), 1)
    from_above = shift(to_below, "x", -1, NX)
    from_below = shift(to_above, "x", 1, NX)
    own = attend_own(pack, [own_kv, *ups[1:], *downs[1:]])
    rec_rows = finish(place, bit, kept, received, out_local, read_f, read_b, rec_gain)
    partials = [own, from_above, from_below, far_low, far_high]
    keep, give = mix(place, rec_rows, partials, lambdas, att_gain)
    got = shift(give, "c", 1, NC)
    joined = join(place, keep, got)
    sources = [joined[0]]
    for k in range(1, NY):
        sources.append(shift(joined[k], "y", k, NY))
    return project(place, sources, out_rec, out_att)


def solution(mesh):
    torus = Mesh(mesh.devices.reshape(NZ, NX, NY, NC), AXES)
    in_specs = (
        P(AXES, None),
        P(),
        P(None, TP),
        P(None, TP),
        P(None, TP),
        P(None, TP),
        P(None, TP),
        P(None, SP, TP),
        P(),
        P(None, TP),
        P(None, TP),
        P(None, TP),
        P(TP),
        P(),
        P(),
        P(),
    )
    out_specs = P(AXES, None)
    return jax.shard_map(
        on_device, mesh=torus, in_specs=in_specs, out_specs=out_specs, check_vma=False
    )
```

```python
import functools

import jax
import jax.numpy as jnp
from jax import lax
from jax.experimental import pallas as pl
from jax.experimental.pallas import tpu as pltpu
from jax.sharding import Mesh
from jax.sharding import PartitionSpec as P


HK = 128
HV = 128
AK = 64
AV = 128
BLOCK = 64
NZ, NX, NY, NC = 8, 4, 4, 2
AXES = ("z", "x", "y", "c")
SP = ("z", "x")
TP = ("y", "c")
TOK = 512
ACC_ROWS = 144
MAP_ROWS = AV + 16
SEND_ROWS = 2 * MAP_ROWS
PACK = 784
BF16 = jnp.bfloat16
F32 = jnp.float32

EPS = 1e-06
THETA = 500000.0
RISE = 40.0
LOW = -1e30
PEERS = NX - 1
FAR = 384


def shift(value, axis, by, size):
    return lax.ppermute(value, axis, [(i, (i + by) % size) for i in range(size)])


def gather_rows(rows):
    half = rows.shape[0] // 2
    far_low = shift(rows[:half], "y", 2, NY)
    far_high = shift(rows[half:], "y", -2, NY)
    up = shift(rows, "y", 1, NY)
    down = shift(rows, "y", -1, NY)
    mine = jnp.concatenate([rows, up, down, far_low, far_high])
    return mine, shift(mine, "c", 1, NC)


def rms_scale(values, gain):
    return values * lax.rsqrt(jnp.mean(values * values, axis=-1, keepdims=True) + EPS) * gain


VMEM = pl.BlockSpec(memory_space=pltpu.VMEM)
SMEM = pl.BlockSpec(memory_space=pltpu.SMEM)


def limit(mib):
    return pltpu.CompilerParams(vmem_limit_bytes=mib << 20)


def cost(flops, transcendentals=0):
    return pl.CostEstimate(flops=flops, transcendentals=transcendentals, bytes_accessed=1 << 20)


def rotation_tables(length):
    positions = (lax.axis_index(SP) * length + jnp.arange(length, dtype=jnp.int32)).astype(F32)
    frequency = THETA ** (-(jnp.arange(AK // 2, dtype=F32) * 2.0 / AK))
    angles = positions[:, None] * frequency[None, :]
    cosine, sine = jnp.cos(angles), jnp.sin(angles)
    return (
        jnp.concatenate([cosine] * 4, axis=1),
        jnp.concatenate([-sine, sine, -sine, sine], axis=1),
    )


def rotated(vectors, cosine, sine):
    lane = lax.broadcasted_iota(jnp.int32, vectors.shape, 1)
    half = AK // 2
    partner = jnp.where(
        (lane & half) == 0, pltpu.roll(vectors, 128 - half, 1), pltpu.roll(vectors, half, 1)
    )
    return vectors * cosine + partner * sine


def keys_body(
    place_ref, mine_ref, other_ref, key_ref, value_ref, cos_ref, sin_ref, rows_ref, out_ref
):
    y, c = place_ref[2], place_ref[3]
    size = mine_ref.shape[0] // NY
    for core, ref in ((c, mine_ref), (1 - c, other_ref)):
        for n, distance in enumerate((0, 3, 1, 2)):
            at = pl.multiple_of((((y + distance) % NY) * NC + core) * size, size)
            rows_ref[pl.ds(at, size), :] = ref[n * size : (n + 1) * size, :]
    weights = jnp.concatenate([key_ref[...], value_ref[...]], axis=1)
    raw = jnp.dot(rows_ref[...], weights, preferred_element_type=F32).astype(BF16)
    out_ref[:TOK, :] = rotated(raw[:, :128].astype(F32), cos_ref[...], sin_ref[...]).astype(BF16)
    for n in range(TOK // 128):
        out_ref[TOK + n * 128 : TOK + (n + 1) * 128, :] = raw[n * 128 : (n + 1) * 128, 128:].T


def make_keys(place, mine, other, key, value, cosine, sine):
    return pl.pallas_call(
        keys_body,
        in_specs=[SMEM] + [VMEM] * 6,
        out_specs=[VMEM, VMEM],
        out_shape=[
            jax.ShapeDtypeStruct((TOK, mine.shape[1]), BF16),
            jax.ShapeDtypeStruct((2 * TOK, 128), BF16),
        ],
        cost_estimate=cost(1 << 29),
        compiler_params=limit(6),
        name="make_keys",
    )(place, mine, other, key, value, cosine, sine)


def local_body(
    rows_ref, aq_ref, q_ref, f_ref, b_ref, v_ref, leak_ref, decay_ref, cos_ref, sin_ref,
    pack_ref, far_a_ref, far_b_ref, out_ref, read_f_ref, read_b_ref,
):
    def project(*weights):
        joined = jnp.concatenate([w[...] for w in weights], axis=1)
        return jnp.dot(rows_ref[...], joined, preferred_element_type=F32).astype(BF16)

    raw_f_b = project(f_ref, b_ref)
    raw_q_v = project(q_ref, v_ref)
    raw_aq = project(aq_ref)
    pack_ref[:TOK, :] = (
        rotated(raw_aq.astype(F32), cos_ref[...], sin_ref[...]) * AK ** (-0.5)
    ).astype(BF16)
    raw = raw_q_v[:, :128].astype(F32)
    queries = raw / (1.0 + jnp.exp(-raw))
    row = lax.broadcasted_iota(jnp.int32, (BLOCK, BLOCK), 0)
    col = lax.broadcasted_iota(jnp.int32, (BLOCK, BLOCK), 1)
    blocks = TOK // BLOCK
    all_keys, all_logs = [], []
    for way in range(2):
        gates = raw_f_b[:, way * HK : (way + 1) * HK].astype(F32)
        keys = leak_ref[way : way + 1, :] / (1.0 + jnp.exp(gates))
        all_keys.append(keys)
        all_logs.append(jnp.log1p(-keys) + decay_ref[way])
    states = [jnp.zeros((HV, HK), F32)] * 2
    befores = [jnp.zeros((1, HK), F32)] * 2
    for step, way in [(step, way) for step in range(blocks) for way in range(2)]:
        n = step if way == 0 else blocks - 1 - step
        keys, logs, state, before = all_keys[way], all_logs[way], states[way], befores[way]
        read_ref = (read_f_ref, read_b_ref)[way]
        reach = (row >= col) if way == 0 else (row <= col)
        sums = jnp.where(reach, 1.0, 0.0)
        middle_row, last_row = (BLOCK // 2 - 1, BLOCK - 1) if way == 0 else (BLOCK // 2, 0)
        at = slice(n * BLOCK, (n + 1) * BLOCK)
        cumulative = jnp.dot(
            sums, logs[at], precision=lax.Precision.HIGHEST, preferred_element_type=F32
        )
        middle = cumulative[middle_row : middle_row + 1]
        last = cumulative[last_row : last_row + 1]
        scores = lax.dot_general(
            (queries[at] * jnp.exp(cumulative - middle)).astype(BF16),
            (keys[at] * jnp.exp(middle - cumulative)).astype(BF16),
            (((1,), (1,)), ((), ())),
            preferred_element_type=F32,
        )
        scores = jnp.where(reach, scores, 0.0).astype(BF16)
        values = raw_q_v[at, 128:]
        out = jnp.dot(scores, values, preferred_element_type=F32)
        read = queries[at] * jnp.exp(cumulative)
        out = out + lax.dot_general(
            read.astype(BF16),
            state.astype(BF16),
            (((1,), (1,)), ((), ())),
            preferred_element_type=F32,
        )
        out_ref[at, :] = out if step < blocks // 2 else out_ref[at, :] + out
        read_ref[at, :] = (read * jnp.exp(before)).astype(BF16)
        added = lax.dot_general(
            values,
            (keys[at] * jnp.exp(last - cumulative)).astype(BF16),
            (((0,), (0,)), ((), ())),
            preferred_element_type=F32,
        )
        states[way] = state * jnp.exp(last) + added
        befores[way] = before + last
    for way in range(2):
        pack_ref[TOK + way * HV : TOK + (way + 1) * HV, :] = states[way].astype(BF16)
    totals = [jnp.exp(before) for before in befores]
    pack_ref[TOK + 2 * HV :, :] = jnp.concatenate(
        [*totals, jnp.zeros((PACK - TOK - 2 * HV - 2, HK), F32)]
    ).astype(BF16)
    far_a_ref[...] = pack_ref[:FAR, :]
    far_b_ref[...] = pack_ref[FAR:, :]


def make_local(rows, weights, leak, decays, cosine, sine):
    return pl.pallas_call(
        local_body,
        in_specs=[VMEM] * 10,
        out_specs=[VMEM] * 6,
        out_shape=[
            jax.ShapeDtypeStruct((PACK, 128), BF16),
            jax.ShapeDtypeStruct((FAR, 128), BF16),
            jax.ShapeDtypeStruct((PACK - FAR, 128), BF16),
            jax.ShapeDtypeStruct((TOK, 128), F32),
            jax.ShapeDtypeStruct((TOK, 128), BF16),
            jax.ShapeDtypeStruct((TOK, 128), BF16),
        ],
        cost_estimate=cost(1 << 31),
        compiler_params=limit(12),
        name="local",
    )(rows, *weights, leak, decays, cosine, sine)


def link(earlier, later):
    return (earlier[0] * later[0], later[0] * earlier[1] + later[1])


def pick(condition, new, old):
    return tuple(jnp.where(condition, a, b) for a, b in zip(new, old))


def read_sent(ref, at):
    decays = ref[at + 2 * HV : at + 2 * HV + 16, :].astype(F32)
    return (
        (decays[0:1], ref[at : at + HV, :].astype(F32)),
        (decays[1:2], ref[at + HV : at + 2 * HV, :].astype(F32)),
    )


def write_sent(ref, fwd, bwd):
    ref[:HV, :] = fwd[1].astype(BF16)
    ref[HV : 2 * HV, :] = bwd[1].astype(BF16)
    ref[2 * HV :, :] = jnp.concatenate([fwd[0], bwd[0], jnp.zeros((14, HK), F32)]).astype(BF16)


def write_kept(ref, n, pair):
    ref[n, :HV, :] = pair[1]
    ref[n, HV:, :] = jnp.broadcast_to(pair[0], (8, HK))


def read_kept(ref, n):
    return ref[n, HV : HV + 1, :], ref[n, :HV, :]


def fold_body(place_ref, own_ref, below1_ref, below2_ref, below3_ref, kept_ref, sent_ref):
    place = place_ref[1]
    entries = [
        read_sent(own_ref, TOK),
        read_sent(below1_ref, TOK),
        read_sent(below2_ref, TOK - FAR),
        read_sent(below3_ref, TOK),
    ]
    none = (jnp.ones((1, HK), F32), jnp.zeros((HV, HK), F32))

    def fold(way, below, order):
        found = none
        for k in order:
            passed = (place >= k) if below else (place < k)
            found = pick(passed, link(found, entries[k][way]), found)
        return found

    f_below, f_above = fold(0, True, (3, 2, 1)), fold(0, False, (3, 2, 1))
    b_above, b_below = fold(1, False, (1, 2, 3)), fold(1, True, (1, 2, 3))
    fwd = link(link(f_below, entries[0][0]), f_above)
    bwd = link(link(b_above, entries[0][1]), b_below)
    for n, pair in enumerate((fwd, bwd, f_below, b_above)):
        write_kept(kept_ref, n, pair)
    write_sent(sent_ref, fwd, bwd)


KEPT = jax.ShapeDtypeStruct((4, HV + 8, HK), F32)
SENT = jax.ShapeDtypeStruct((2 * HV + 16, HK), BF16)


def fold_x(place, packs):
    return pl.pallas_call(
        fold_body,
        in_specs=[SMEM] + [VMEM] * 4,
        out_specs=[VMEM, VMEM],
        out_shape=[KEPT, SENT],
        cost_estimate=cost(1 << 22),
        compiler_params=limit(4),
        name="fold_x",
    )(place, *packs)


def is_lower(place_ref, bit):
    return (place_ref[0] & bit) != 0


def met(lower, kept_ref, received_ref):
    fwd, bwd, before, after = (read_kept(kept_ref, n) for n in range(4))
    peer_f, peer_b = read_sent(received_ref, 0)
    return (
        pick(lower, link(peer_f, fwd), link(fwd, peer_f)),
        pick(lower, link(bwd, peer_b), link(peer_b, bwd)),
        pick(lower, link(peer_f, before), before),
        pick(lower, after, link(peer_b, after)),
    )


def merge_body(place_ref, kept_ref, received_ref, out_ref, sent_ref, *, bit):
    pairs = met(is_lower(place_ref, bit), kept_ref, received_ref)
    for n, pair in enumerate(pairs):
        write_kept(out_ref, n, pair)
    write_sent(sent_ref, pairs[0], pairs[1])


def merge(place, bit, kept, received):
    return pl.pallas_call(
        functools.partial(merge_body, bit=bit),
        in_specs=[SMEM, VMEM, VMEM],
        out_specs=[VMEM, VMEM],
        out_shape=[KEPT, SENT],
        cost_estimate=cost(1 << 22),
        compiler_params=limit(4),
        name="merge",
    )(place, kept, received)


def finish_body(
    place_ref, kept_ref, received_ref, out_ref, read_f_ref, read_b_ref, gain_ref, rows_ref, *, bit
):
    _, _, before, after = met(is_lower(place_ref, bit), kept_ref, received_ref)
    total = out_ref[...]
    for read_ref, (_, state) in ((read_f_ref, before), (read_b_ref, after)):
        total = total + lax.dot_general(
            read_ref[...], state.astype(BF16), (((1,), (1,)), ((), ())), preferred_element_type=F32
        )
    rows_ref[...] = rms_scale(total, gain_ref[...]).astype(BF16)


def finish(place, bit, kept, received, out, read_f, read_b, gain):
    return pl.pallas_call(
        functools.partial(finish_body, bit=bit),
        in_specs=[SMEM] + [VMEM] * 6,
        out_specs=VMEM,
        out_shape=jax.ShapeDtypeStruct((TOK, HV), BF16),
        cost_estimate=cost(1 << 25),
        compiler_params=limit(4),
        name="finish",
    )(place, kept, received, out, read_f, read_b, gain.reshape(1, HV))


def attend_tile(maps, kv_refs, peaks, accs):
    ones = jnp.ones((ACC_ROWS - AV, TOK), BF16)
    values = [
        jnp.concatenate(
            [
                jnp.concatenate(
                    [kv[TOK + n * 128 : TOK + (n + 1) * 128, :] for n in range(TOK // 128)], axis=1
                ),
                ones,
            ]
        )
        for kv in kv_refs
    ]
    accs, peaks, rises = list(accs), list(peaks), []
    units = [(m, n) for m in range(len(maps)) for n in range(len(kv_refs))]

    def scores_of(unit):
        return jnp.dot(kv_refs[unit[1]][:TOK, :], maps[unit[0]], preferred_element_type=F32)

    scores = scores_of(units[0])
    for at, (m, n) in enumerate(units):
        upcoming = scores_of(units[at + 1]) if at + 1 < len(units) else None
        found = peaks[m] is None
        if found:
            peaks[m] = jnp.max(scores, axis=0, keepdims=True)
        above = scores - peaks[m]
        if not found:
            rises.append(jnp.max(above.reshape(-1, 8, above.shape[1]), axis=0))
        added = jnp.dot(values[n], jnp.exp(above).astype(BF16), preferred_element_type=F32)
        accs[m] = added if accs[m] is None else accs[m] + added
        scores = upcoming
    return accs, peaks, jnp.max(functools.reduce(jnp.maximum, rises)) if rises else None


def attend_again(maps_ref, kv_refs, peaks_ref, accs_ref):
    ones = jnp.ones((ACC_ROWS - AV, 128), BF16)
    steps = TOK // 128
    for kv in kv_refs:

        def absorb(i, unused):
            m, w, n = i // (steps * steps), (i // steps) % steps, i % steps
            keys = kv[pl.ds(pl.multiple_of(n * 128, 128), 128), :]
            values = kv[pl.ds(pl.multiple_of(TOK + n * 128, 128), 128), :]
            cols = pl.ds(pl.multiple_of(w * 128, 128), 128)
            scores = jnp.dot(keys, maps_ref[m, :, cols], preferred_element_type=F32)
            old = peaks_ref[m, 0:1, cols]
            new = jnp.maximum(old, jnp.max(scores, axis=0, keepdims=True))
            accs_ref[m, :, cols] = accs_ref[m, :, cols] * jnp.exp(old - new) + jnp.dot(
                jnp.concatenate([values, ones]),
                jnp.exp(scores - new).astype(BF16),
                preferred_element_type=F32,
            )
            peaks_ref[m, 0:1, cols] = new
            return 0

        lax.fori_loop(0, 2 * steps * steps, absorb, 0)


def both_maps(turned):
    upper = lax.broadcasted_iota(jnp.int32, turned.shape, 0) < AK
    zero = jnp.zeros_like(turned)
    return jnp.where(upper, turned, zero), jnp.where(upper, zero, turned)


def attend_first_body(below_ref, above_ref, far_a_ref, far_b_ref, kv_ref, turned_ref, peaks_ref, accs_ref):
    turned_ref[0] = below_ref[:TOK, :].T
    turned_ref[1] = above_ref[:TOK, :].T
    turned_ref[2] = jnp.concatenate([far_a_ref[...], far_b_ref[: TOK - FAR, :]]).T

    def tile(t, unused):
        accs, peaks, _ = attend_tile(both_maps(turned_ref[t]), [kv_ref], [None] * 2, [None] * 2)
        for m in range(2):
            accs_ref[t, m] = accs[m]
            peaks_ref[t, m] = jnp.broadcast_to(peaks[m], (8, TOK))
        return 0

    lax.fori_loop(0, PEERS, tile, 0)


def attend_more_body(turned_ref, *refs, chunks):
    kv_refs, (peaks_in, accs_in, peaks_ref, accs_ref, maps_ref) = refs[:chunks], refs[chunks:]
    peaks_ref[...] = peaks_in[...]

    def tile(t, unused):
        maps = both_maps(turned_ref[t])
        peaks = [peaks_in[t, m, 0:1, :] for m in range(2)]
        accs, _, rise = attend_tile(maps, kv_refs, peaks, [accs_in[t, m] for m in range(2)])
        for m in range(2):
            accs_ref[t, m] = accs[m]

        @pl.when(rise > RISE)
        def _():
            maps_ref[0], maps_ref[1] = maps
            accs_ref[t] = accs_in[t]
            attend_again(maps_ref, kv_refs, peaks_ref.at[t], accs_ref.at[t])

        return 0

    lax.fori_loop(0, PEERS, tile, 0)


def write_partial(send_refs, peaks_ref, accs_ref):
    for m in range(2):
        acc = accs_ref[m]
        total = acc[AV : AV + 1, :]
        level = peaks_ref[m, 0:1, :] + jnp.log(total)
        high = level.astype(BF16)
        left = level - high.astype(F32)
        middle = left.astype(BF16)
        low = (left - middle.astype(F32)).astype(BF16)
        mean = (acc[:AV] * (1.0 / total)).astype(BF16)
        levels = jnp.concatenate(
            [high.astype(F32), middle.astype(F32), low.astype(F32), jnp.zeros((13, TOK), F32)]
        ).astype(BF16)
        ref = send_refs[m] if len(send_refs) > 1 else send_refs[0]
        at = 0 if len(send_refs) > 1 else m * MAP_ROWS
        ref[at : at + AV, :] = mean
        ref[at + AV : at + MAP_ROWS, :] = levels


def attend_last_body(turned_ref, *refs, chunks, tiles):
    kv_refs, rest = refs[:chunks], refs[chunks:]
    peaks_in, accs_in, *send_refs, peaks_ref, accs_ref, maps_ref, rise_ref = rest
    start, count = tiles
    for t in range(count):
        maps_ref[t, 0], maps_ref[t, 1] = both_maps(turned_ref[start + t])
        rise_ref[t] = 0.0

    def one_map(i, unused):
        t, m = i // 2, i % 2
        peaks = peaks_in[start + t, m]
        accs, _, rise = attend_tile(
            [maps_ref[t, m]], kv_refs, [peaks[0:1]], [accs_in[start + t, m]]
        )
        peaks_ref[t, m] = peaks
        accs_ref[t, m] = accs[0]
        rise_ref[t] = jnp.maximum(rise_ref[t], rise)
        return 0

    lax.fori_loop(0, 2 * count, one_map, 0)

    def check(t, unused):
        @pl.when(rise_ref[t] > RISE)
        def _():
            accs_ref[t] = accs_in[start + t]
            attend_again(maps_ref.at[t], kv_refs, peaks_ref.at[t], accs_ref.at[t])

        return 0

    lax.fori_loop(0, count, check, 0)
    parts = len(send_refs) // count
    for t in range(count):
        write_partial(send_refs[t * parts : (t + 1) * parts], peaks_ref.at[t], accs_ref.at[t])


def attend_own_body(pack_ref, *refs, chunks):
    kv_refs, (own_ref, peaks_ref, accs_ref, maps_ref, rise_ref) = refs[:chunks], refs[chunks:]
    maps_ref[0, 0], maps_ref[0, 1] = both_maps(pack_ref[:TOK, :].T)
    rise_ref[0] = 0.0

    def one_map(m, unused):
        accs, peaks, rise = attend_tile([maps_ref[0, m]], kv_refs, [None], [None])
        accs_ref[0, m] = accs[0]
        peaks_ref[0, m] = jnp.broadcast_to(peaks[0], (8, TOK))
        rise_ref[0] = jnp.maximum(rise_ref[0], rise)
        return 0

    lax.fori_loop(0, 2, one_map, 0)

    @pl.when(rise_ref[0] > RISE)
    def _():
        peaks_ref[...] = jnp.full(peaks_ref.shape, LOW, F32)
        accs_ref[...] = jnp.zeros(accs_ref.shape, F32)
        attend_again(maps_ref.at[0], kv_refs, peaks_ref.at[0], accs_ref.at[0])

    write_partial([own_ref], peaks_ref.at[0], accs_ref.at[0])


STATE = [
    jax.ShapeDtypeStruct((PEERS, 2, 8, TOK), F32),
    jax.ShapeDtypeStruct((PEERS, 2, ACC_ROWS, TOK), F32),
]


def tile_scratch(count):
    return [
        pltpu.VMEM((count, 2, 8, TOK), F32),
        pltpu.VMEM((count, 2, ACC_ROWS, TOK), F32),
        pltpu.VMEM((count, 2, 2 * AK, TOK), BF16),
        pltpu.SMEM((count,), F32),
    ]


def attend_cost(tiles, chunks):
    work = 2 * tiles * TOK * chunks * TOK
    return cost(work * 2 * (AK + AV), work)


def attend_first(*operands):
    return pl.pallas_call(
        attend_first_body,
        in_specs=[VMEM] * 5,
        out_specs=[VMEM] * 3,
        out_shape=[jax.ShapeDtypeStruct((PEERS, 2 * AK, TOK), BF16), *STATE],
        cost_estimate=attend_cost(PEERS, 1),
        compiler_params=limit(14),
        name="attend_first",
    )(*operands)


def attend_more(turned, pieces, state):
    return pl.pallas_call(
        functools.partial(attend_more_body, chunks=len(pieces)),
        in_specs=[VMEM] * (len(pieces) + 3),
        out_specs=[VMEM] * 2,
        out_shape=STATE,
        scratch_shapes=[pltpu.VMEM((2, 2 * AK, TOK), BF16)],
        cost_estimate=attend_cost(PEERS, len(pieces)),
        compiler_params=limit(14),
        name="attend_more",
    )(turned, *pieces, *state)


def attend_last(turned, pieces, state, tiles, parts):
    count = tiles[1]
    return pl.pallas_call(
        functools.partial(attend_last_body, chunks=len(pieces), tiles=tiles),
        in_specs=[VMEM] * (len(pieces) + 3),
        out_specs=[VMEM] * (parts * count),
        out_shape=[jax.ShapeDtypeStruct((SEND_ROWS // parts, TOK), BF16)] * (parts * count),
        scratch_shapes=tile_scratch(count),
        cost_estimate=attend_cost(count, len(pieces)),
        compiler_params=limit(14),
        name="attend_last",
    )(turned, *pieces, *state)


def attend_own(pack, pieces):
    return pl.pallas_call(
        functools.partial(attend_own_body, chunks=len(pieces)),
        in_specs=[VMEM] * (len(pieces) + 1),
        out_specs=VMEM,
        out_shape=jax.ShapeDtypeStruct((SEND_ROWS, TOK), BF16),
        scratch_shapes=tile_scratch(1),
        cost_estimate=attend_cost(1, len(pieces)),
        compiler_params=limit(14),
        name="attend_own",
    )(pack, *pieces)


SWAP = TOK // (NY * NC)


def mix_body(
    place_ref, rec_ref, a_ref, b_ref, c_ref, low_ref, high_ref, weight_ref, gain_ref,
    keep_ref, give_ref, att_ref,
):
    mixed = None
    for m in range(2):
        places = [(ref, m * MAP_ROWS) for ref in (a_ref, b_ref, c_ref)]
        places.append(((low_ref, high_ref)[m], 0))
        levels = []
        for ref, at in places:
            parts = ref[at + AV : at + MAP_ROWS, :].astype(F32)
            levels.append(parts[0:1] + parts[1:2] + parts[2:3])
        peak = functools.reduce(jnp.maximum, levels)
        shares = [jnp.exp(level - peak) for level in levels]
        scale = 1.0 / functools.reduce(jnp.add, shares)
        if m == 1:
            scale = scale * -weight_ref[0]
        for (ref, at), share in zip(places, shares):
            term = ref[at : at + AV, :].astype(F32) * (share * scale)
            mixed = term if mixed is None else mixed + term
    scale = lax.rsqrt(jnp.mean(mixed * mixed, axis=0, keepdims=True) + EPS)
    att_ref[...] = ((mixed * scale).T * gain_ref[...]).astype(BF16)
    y, c = place_ref[2], place_ref[3]
    for ref, core in ((keep_ref, c), (give_ref, 1 - c)):
        for k in range(NY):
            at = pl.multiple_of((((y + k) % NY) * NC + core) * SWAP, SWAP)
            ref[k, :, :HV] = rec_ref[pl.ds(at, SWAP), :]
            ref[k, :, HV:] = att_ref[pl.ds(at, SWAP), :]


def mix(place, rec_rows, partials, weight, gain):
    half = jax.ShapeDtypeStruct((NY, SWAP, HV + AV), BF16)
    return pl.pallas_call(
        mix_body,
        in_specs=[SMEM] + [VMEM] * 6 + [SMEM, VMEM],
        out_specs=[VMEM] * 2,
        out_shape=[half, half],
        scratch_shapes=[pltpu.VMEM((TOK, AV), BF16)],
        cost_estimate=cost(1 << 22),
        compiler_params=limit(6),
        name="mix",
    )(place, rec_rows, *partials, weight, gain.reshape(1, AV))


def join_body(place_ref, keep_ref, got_ref, *out_refs):
    first = place_ref[3] == 0
    for k, ref in enumerate(out_refs):
        keep, got = keep_ref[k], got_ref[k]
        low, high = jnp.where(first, keep, got), jnp.where(first, got, keep)
        ref[:, :HV], ref[:, HV : 2 * HV] = low[:, :HV], high[:, :HV]
        ref[:, 2 * HV : 2 * HV + AV], ref[:, 2 * HV + AV :] = low[:, HV:], high[:, HV:]


def join(place, keep, got):
    return pl.pallas_call(
        join_body,
        in_specs=[SMEM, VMEM, VMEM],
        out_specs=[VMEM] * NY,
        out_shape=[jax.ShapeDtypeStruct((SWAP, 2 * (HV + AV)), BF16)] * NY,
        cost_estimate=cost(1 << 20),
        compiler_params=limit(2),
        name="join",
    )(place, keep, got)


def project_body(place_ref, *refs):
    sources, (rec_ref, att_ref, out_ref, rows_ref) = refs[:NY], refs[NY:]
    for k, ref in enumerate(sources):
        at = pl.multiple_of(((place_ref[2] + NY - k) % NY) * 2 * HV, 2 * HV)
        for n in range(2):
            rows_ref[n, :, pl.ds(at, 2 * HV)] = ref[:, n * 2 * HV : (n + 1) * 2 * HV]
    total = jnp.dot(rows_ref[0], rec_ref[...], preferred_element_type=F32)
    total = total + jnp.dot(rows_ref[1], att_ref[...], preferred_element_type=F32)
    out_ref[...] = total.astype(BF16)


def project(place, sources, out_rec, out_att):
    return pl.pallas_call(
        project_body,
        in_specs=[SMEM] + [VMEM] * (NY + 2),
        out_specs=VMEM,
        out_shape=jax.ShapeDtypeStruct((SWAP, out_rec.shape[1]), BF16),
        scratch_shapes=[pltpu.VMEM((2, SWAP, 2 * NY * HV), BF16)],
        cost_estimate=cost(1 << 29),
        compiler_params=limit(6),
        name="project",
    )(place, *sources, out_rec, out_att)


def on_device(
    tokens,
    norm_gain,
    rec_query,
    fwd_gate,
    bwd_gate,
    rec_value,
    gate_leak,
    log_decay,
    rec_gain,
    att_query,
    att_key,
    att_value,
    lambdas,
    att_gain,
    out_rec,
    out_att,
):
    place = jnp.stack([lax.axis_index(axis) for axis in AXES]).astype(jnp.int32)
    decays = jnp.broadcast_to(log_decay, (2, TOK, 128))
    cosine, sine = rotation_tables(TOK)
    normed = rms_scale(tokens.astype(F32), norm_gain).astype(BF16)
    mine, other = gather_rows(normed)
    rows, own_kv = make_keys(place, mine, other, att_key, att_value, cosine, sine)
    ups, downs = [own_kv], [own_kv]
    for step in range(1, NZ // 2 + 1):
        ups.append(shift(ups[-1], "z", 1, NZ))
        if step < NZ // 2:
            downs.append(shift(downs[-1], "z", -1, NZ))
    pack, far_a, far_b, out_local, read_f, read_b = make_local(
        rows,
        (att_query, rec_query, fwd_gate, bwd_gate, rec_value),
        gate_leak,
        decays,
        cosine,
        sine,
    )
    far_a = shift(far_a, "x", 2, NX)
    far_b = shift(far_b, "x", -2, NX)
    below = shift(pack, "x", 1, NX)
    above = shift(pack, "x", -1, NX)
    kept, sent = fold_x(place, [pack, below, far_b, above])
    turned, *state = attend_first(below, above, far_a, far_b, own_kv)
    for bit in (1, 2, 4):
        received = lax.ppermute(sent, "z", [(i, i ^ bit) for i in range(NZ)])
        if bit < 4:
            kept, sent = merge(place, bit, kept, received)
    state = attend_more(turned, [ups[1], downs[1]], state)
    state = attend_more(turned, [ups[2], downs[2]], state)
    ends = [ups[3], downs[3], ups[4]]
    low, high = attend_last(turned, ends, state, (2, 1), 2)
    far_low = shift(low, "x", 2, NX)
    far_high = shift(high, "x", -2, NX)
    to_below, to_above = attend_last(turned, ends, state, (0, 2), 1)
    from_above = shift(to_below, "x", -1, NX)
    from_below = shift(to_above, "x", 1, NX)
    own = attend_own(pack, [own_kv, *ups[1:], *downs[1:]])
    rec_rows = finish(place, bit, kept, received, out_local, read_f, read_b, rec_gain)
    partials = [own, from_above, from_below, far_low, far_high]
    keep, give = mix(place, rec_rows, partials, lambdas, att_gain)
    got = shift(give, "c", 1, NC)
    joined = join(place, keep, got)
    sources = [joined[0]]
    for k in range(1, NY):
        sources.append(shift(joined[k], "y", k, NY))
    return project(place, sources, out_rec, out_att)


def solution(mesh):
    torus = Mesh(mesh.devices.reshape(NZ, NX, NY, NC), AXES)
    in_specs = (
        P(AXES, None),
        P(),
        P(None, TP),
        P(None, TP),
        P(None, TP),
        P(None, TP),
        P(None, TP),
        P(None, SP, TP),
        P(),
        P(None, TP),
        P(None, TP),
        P(None, TP),
        P(TP),
        P(),
        P(),
        P(),
    )
    out_specs = P(AXES, None)
    return jax.shard_map(
        on_device, mesh=torus, in_specs=in_specs, out_specs=out_specs, check_vma=False
    )
```
